256 devices in a mesh: fs: 16 (over y, x), tp: 16 (over z, core).
Axes of the slice: x: 4, y: 4, z: 8, core: 2. Of those that a mesh axis runs over, the one named last changes fastest.
Arguments:
- tokens: bfloat16 [32768, 2048], P(('fs', 'tp')), may hold values from -6 to 6
- norm_gain: float32 [2048], replicated, may hold values from 0.1 to 1.9
- gate_weight: bfloat16 [2048, 5632], P('fs', 'tp'), may hold values from -0.125 to 0.125
- up_weight: bfloat16 [2048, 5632], P('fs', 'tp'), may hold values from -0.125 to 0.125
- down_weight: bfloat16 [5632, 2048], P('tp', 'fs'), may hold values from -0.078125 to 0.078125
Outputs:
- mixed: bfloat16 [32768, 2048], P(('fs', 'tp'))
The draws below stay inside these ranges and needn't reach their ends.
All inputs are finite; a program needn't handle non-finite values.
Results may differ from the reference program's by a relative error of at most 0.0065.
Values may be sent and summed in bfloat16 or wider, within the bound.
A program may use at most 128 MiB of HBM per device.

```python
import jax
import jax.numpy as jnp
from jax import lax

D = 2048
FF = 5632
TOK_DEV = 128
TOKENS = 32768


def shard_levels(stream_key, extent, pieces, low, high):
    factor_of = 1.0
    for dim, blocks in pieces:
        draws = jax.random.uniform(jax.random.fold_in(jax.random.fold_in(stream_key, 6), dim), (blocks,), jnp.float32, low / len(pieces), high / len(pieces))
        factor_of = factor_of * jnp.repeat(jnp.exp(draws), extent[dim] // blocks).reshape((-1,) + (1,) * (len(extent) - 1 - dim))
    return factor_of


def centred(key, dims, scale, limit, cuts=(), held_as=jnp.bfloat16):
    loudness = shard_levels(key, dims, cuts, -0.22, 0.18) if cuts else 1.0
    entries = jax.random.normal(key, dims, jnp.float32) * scale * loudness
    return jnp.minimum(jnp.maximum(entries, -limit), limit).astype(held_as)


def setup_inputs(seed: int = 0) -> dict:
    streams_of = jax.random.split(jax.random.key(seed), 6)
    return {
        "tokens": centred(streams_of[0], (TOKENS, D), 1.0, 6.0, ((0, 256),)),
        "norm_gain": jnp.clip(1.0 + 0.18 * jax.random.normal(streams_of[1], (D,), jnp.float32), 0.1, 1.9),
        "gate_weight": centred(streams_of[2], (D, FF), D ** -0.5, 0.125, ((0, 16), (1, 16))),
        "up_weight": centred(streams_of[3], (D, FF), D ** -0.5, 0.125, ((0, 16), (1, 16))),
        "down_weight": centred(streams_of[4], (FF, D), FF ** -0.5, 0.078125, ((0, 16), (1, 16))),
    }


eps_floor = 0.05

def reference(tokens, norm_gain, gate_weight, up_weight, down_weight):
    blocks = tokens.reshape(-1, TOK_DEV, D)

    def one_block(rows):
        values = rows.astype(jnp.float32)
        factor = lax.rsqrt(lax.optimization_barrier(jnp.mean(values * values, axis=-1, keepdims=True)) + eps_floor)
        normed = (values * factor * norm_gain).astype(jnp.bfloat16)
        gate = jnp.dot(normed, gate_weight, preferred_element_type=jnp.float32)
        upper = jnp.dot(normed, up_weight, preferred_element_type=jnp.float32)
        hidden = (jax.nn.silu(gate) * upper).astype(jnp.bfloat16)
        return jnp.dot(hidden, down_weight, preferred_element_type=jnp.float32).astype(jnp.bfloat16)
    return lax.map(one_block, blocks).reshape(TOKENS, D)
```

```python
import jax
import jax.numpy as jnp
from jax import lax
from jax.experimental import pallas as pl
from jax.experimental.pallas import tpu as pltpu
from jax.sharding import PartitionSpec as P

MESH = pl.DeviceIdType.MESH
BF, F32 = jnp.bfloat16, jnp.float32
eps_floor = 0.05

D, T, HU, HP = 2048, 128, 352, 384
GU_A, GU_B, D_A, D_B = 0, 1, 2, 3
PAIRS = (
    ((0, 0), (0, 1)),
    ((0, -1), (1, 0)),
    ((-1, 0), (2, 0)),
    ((1, 1), (1, -1)),
    ((-1, 1), (-1, -1)),
    ((0, 2), (1, 2)),
    ((-1, 2), (2, 1)),
    ((2, -1), (2, 2)),
)


def kernel(tok, gain, gate, up, down, out, wg, wd, x4, nrm, acc, hid, pb, rb, own, stage,
           in_sem, ssem, rsem, dsend, drecv_g, drecv_d, zsend, zrecv, tsend, trecv, psend, precv):
    fs, tp = lax.axis_index("fs"), lax.axis_index("tp")
    y, x, z, c = fs // 4, fs % 4, tp // 2, tp % 2
    d = 1 - 2 * c
    par = (x + y) % 2
    pars = (par, 1 - par, 1 - par, par)
    sibling = (fs, z * 2 + 1 - c)

    def zdev(k):
        return (fs, ((z + k + 8) % 8) * 2 + c)

    def fpos(t, i, j):
        p = pars[t]
        yy = (y + i * p + j * (1 - p) + 8) % 4
        xx = (x + i * (1 - p) + j * p + 8) % 4
        return yy * 4 + xx

    def piece(t, core, f):
        if t < 2:
            return wg.at[core, t, f]
        return wd.at[f, core * 2 + (t - 2), pl.ds(0, HU), :]

    def rcopy(src, dst, s, r, dev):
        return pltpu.make_async_remote_copy(
            src_ref=src, dst_ref=dst, send_sem=s, recv_sem=r, device_id=dev, device_id_type=MESH
        )

    def send(t, src, to):
        f = fpos(t, *src)
        ref = piece(t, c, f)
        rcopy(ref, ref, ssem.at[t], rsem.at[t, f], (fpos(t, *to), tp)).start()

    def across(t, src):
        f = fpos(t, *src)
        ref = piece(t, c, f)
        r = drecv_g.at[t] if t < 2 else drecv_d.at[t - 2, f]
        rcopy(ref, ref, dsend.at[t], r, sibling).start()

    def got(t, src):
        f = fpos(t, *src)
        ref = piece(t, c, f)
        rcopy(ref, ref, ssem.at[t], rsem.at[t, f], sibling).wait_recv()

    def s1(t):
        for to in ((1, 0), (-1, 0), (0, 1), (0, -1)):
            send(t, (0, 0), to)
        across(t, (0, 0))

    def s2(t):
        got(t, (0, -d))
        send(t, (0, -d), (0, d))
        send(t, (0, -d), (1, 0))
        send(t, (0, -d), (-1, 0))
        got(t, (0, d))
        send(t, (0, d), (1, 0))
        send(t, (0, d), (-1, 0))
        got(t, (-d, 0))
        send(t, (-d, 0), (d, 0))
        got(t, (d, 0))
        for src in ((0, -d), (0, d), (-d, 0), (d, 0)):
            across(t, src)

    def s3(t):
        got(t, (2, 0))
        send(t, (2, 0), (0, 1))
        send(t, (2, 0), (0, -1))
        for i in (1, -1):
            got(t, (i, -d))
            send(t, (i, -d), (0, d))
        for src in ((1, d), (-1, d), (0, 2)):
            got(t, src)
        for src in ((2, 0), (1, -d), (-1, -d), (1, d), (-1, d), (0, 2)):
            across(t, src)

    def s4(t):
        got(t, (-d, 2))
        send(t, (-d, 2), (d, 0))
        for src in ((d, 2), (2, 1), (2, -1)):
            got(t, src)
        for src in ((-d, 2), (d, 2), (2, 1), (2, -1)):
            across(t, src)

    def s5(t):
        got(t, (2, 2))
        across(t, (2, 2))

    def normalize(slot):
        def rows(i, _):
            at = pl.multiple_of(i * 16, 16)
            v = x4[slot, pl.ds(at, 16), :].astype(F32)
            factor = lax.rsqrt(jnp.sum(v * v, axis=-1, keepdims=True) * (1.0 / D) + eps_floor)
            nrm[pl.ds(pl.multiple_of(slot * T + at, 16), 16), :] = (v * factor * gain[...]).astype(BF)
            return 0

        lax.fori_loop(0, T // 16, rows, 0)

    def gate_up(core, ab):
        def columns(n, _):
            at = pl.multiple_of(n * 256, 256)
            w = wg[core, ab, :, :, pl.ds(at, 256)].reshape(D, 256)
            acc[:, pl.ds(at, 256)] = jnp.dot(nrm[...], w, preferred_element_type=F32)
            return 0

        lax.fori_loop(0, 3, columns, 0)
        lanes = pl.ds(pl.multiple_of((core * 2 + ab) * HP, 128), HP)

        def rows(i, _):
            at = pl.ds(pl.multiple_of(i * 32, 32), 32)
            g = acc[at, 0:HP]
            u = acc[at, HP : 2 * HP]
            hid[at, lanes] = (g / (1.0 + jnp.exp(-g)) * u).astype(BF)
            return 0

        lax.fori_loop(0, 16, rows, 0)

    def pair_fs(p):
        return [fpos(D_A, *o) for o in PAIRS[p]]

    def down_pair(p):
        fa, fb = pair_fs(p)
        for t in (D_A, D_B):
            for f in (fa, fb):
                ref = piece(t, 1 - c, f)
                rcopy(ref, ref, dsend.at[t], drecv_d.at[t - 2, f], sibling).wait_recv()
        w = jnp.concatenate([wd[fa].reshape(4 * HP, 128), wd[fb].reshape(4 * HP, 128)], axis=1)
        part = jnp.dot(hid[...], w, preferred_element_type=F32)
        for s in (1, 2, 3):
            for h in (0, 1):
                pb[p, s - 1, h] = part[s * T : (s + 1) * T, h * 128 : (h + 1) * 128].astype(BF)
        own[p] = part[0:T]
        for s, k in ((3, -2 * d), (1, -d), (2, d)):
            rcopy(pb.at[p, s - 1], rb.at[s - 1, p], psend, precv.at[s - 1, p], zdev(k)).start()

    def finish(p):
        for s in (0, 1, 2):
            rcopy(rb.at[s, p], rb.at[s, p], psend, precv.at[s, p], sibling).wait_recv()
        for h, f in enumerate(pair_fs(p)):
            v = own[p, :, h * 128 : (h + 1) * 128]
            for s in (0, 1, 2):
                v = v + rb[s, p, h].astype(F32)
            out[:, pl.ds(pl.multiple_of(f * 128, 128), 128)] = v.astype(BF)

    gd = pltpu.make_async_copy(gate, stage.at[0], in_sem.at[0])
    ud = pltpu.make_async_copy(up, stage.at[1], in_sem.at[1])
    dd = pltpu.make_async_copy(down, piece(D_A, c, fs), in_sem.at[2])
    td = pltpu.make_async_copy(tok, x4.at[0], in_sem.at[3])
    for cp in (gd, ud, dd, td):
        cp.start()
    barrier = pltpu.get_barrier_semaphore()
    partners = [sibling] + [(fpos(0, *o), tp) for o in ((1, 0), (-1, 0), (0, 1), (0, -1))]
    partners += [zdev(k) for k in (1, -1, 2, -2, 4)]
    for dev in partners:
        pl.semaphore_signal(barrier, inc=1, device_id=dev, device_id_type=MESH)
    for f in range(16):
        for b in range(4):
            wd[f, b, HU:HP, :] = jnp.zeros((HP - HU, 128), BF)
    gd.wait()
    ud.wait()
    pad = jnp.zeros((T, HP - HU), BF)
    wg[c, 0, fs, :, 0:HP] = jnp.concatenate([stage[0], pad], axis=1)
    wg[c, 0, fs, :, HP : 2 * HP] = jnp.concatenate([stage[1], pad], axis=1)
    dd.wait()
    td.wait()
    pl.semaphore_wait(barrier, len(partners))

    s1(GU_A)
    gz = rcopy(piece(GU_A, c, fs), piece(GU_B, c, fs), zsend.at[0], zrecv.at[0], zdev(4))
    gz.start()
    t2 = rcopy(x4.at[0], x4.at[2], tsend, trecv.at[2], zdev(-d))
    t1 = rcopy(x4.at[0], x4.at[1], tsend, trecv.at[1], zdev(d))
    t3 = rcopy(x4.at[1], x4.at[3], tsend, trecv.at[3], zdev(d))
    dz = rcopy(piece(D_A, c, fs), piece(D_B, c, fs), zsend.at[1], zrecv.at[1], zdev(4))
    t2.start()
    t1.start()
    s1(D_A)
    s2(GU_A)
    gz.wait_recv()
    s1(GU_B)
    s2(D_A)
    t1.wait_recv()
    t3.start()
    dz.start()
    s3(GU_A)
    s2(GU_B)
    s4(GU_A)
    s3(GU_B)
    s5(GU_A)
    normalize(0)
    normalize(1)
    s4(GU_B)
    dz.wait_recv()
    s1(D_B)
    s3(D_A)
    t2.wait_recv()
    normalize(2)
    t3.wait_recv()
    normalize(3)
    rcopy(wg.at[1 - c, 0], wg.at[1 - c, 0], dsend.at[0], drecv_g.at[0], sibling).wait_recv()
    gate_up(c, 0)
    s2(D_B)
    s4(D_A)
    gate_up(1 - c, 0)
    s5(GU_B)
    gate_up(c, 1)
    s3(D_B)
    s5(D_A)
    rcopy(wg.at[1 - c, 1], wg.at[1 - c, 1], dsend.at[1], drecv_g.at[1], sibling).wait_recv()
    gate_up(1 - c, 1)
    s4(D_B)
    down_pair(0)
    down_pair(1)
    s5(D_B)
    for p in range(2, 8):
        down_pair(p)
        finish(p - 2)
    finish(6)
    finish(7)

    for t in (GU_A, GU_B):
        few = wg.at[c, t, pl.ds(0, 15)]
        rcopy(few, few, ssem.at[t], rsem.at[t, 0], sibling).wait_send()
        rcopy(wg.at[c, t], wg.at[c, t], dsend.at[t], drecv_g.at[t], sibling).wait_send()
    for t in (D_A, D_B):
        few = wd.at[pl.ds(0, 15), 0, pl.ds(0, HU), :]
        rcopy(few, few, ssem.at[t], rsem.at[t, 0], sibling).wait_send()
        all16 = wd.at[:, 0, pl.ds(0, HU), :]
        rcopy(all16, all16, dsend.at[t], drecv_d.at[t - 2, 0], sibling).wait_send()
    gz.wait_send()
    dz.wait_send()
    three = x4.at[pl.ds(0, 3)]
    rcopy(three, three, tsend, trecv.at[1], sibling).wait_send()
    rcopy(pb, pb, psend, precv.at[0, 0], sibling).wait_send()


def local(tokens, norm_gain, gate_weight, up_weight, down_weight):
    hbm = pl.BlockSpec(memory_space=pl.ANY)
    vmem = pl.BlockSpec(memory_space=pltpu.VMEM)
    dma = pltpu.SemaphoreType.DMA
    return pl.pallas_call(
        kernel,
        out_shape=jax.ShapeDtypeStruct((T, D), BF),
        in_specs=[hbm, vmem, hbm, hbm, hbm],
        out_specs=vmem,
        scratch_shapes=[
            pltpu.VMEM((2, 2, 16, 128, 2 * HP), BF),
            pltpu.VMEM((16, 4, HP, 128), BF),
            pltpu.VMEM((4, T, D), BF),
            pltpu.VMEM((4 * T, D), BF),
            pltpu.VMEM((4 * T, 2 * HP), F32),
            pltpu.VMEM((4 * T, 4 * HP), BF),
            pltpu.VMEM((8, 3, 2, T, 128), BF),
            pltpu.VMEM((3, 8, 2, T, 128), BF),
            pltpu.VMEM((8, T, 256), F32),
            pltpu.VMEM((2, 128, HU), BF),
            dma((4,)),
            dma((4,)),
            dma((4, 16)),
            dma((4,)),
            dma((2,)),
            dma((2, 16)),
            dma((2,)),
            dma((2,)),
            dma(()),
            dma((4,)),
            dma(()),
            dma((3, 8)),
        ],
        compiler_params=pltpu.CompilerParams(
            collective_id=0, has_side_effects=True, vmem_limit_bytes=58 * 2**20
        ),
    )(tokens, norm_gain.reshape(1, D), gate_weight, up_weight, down_weight)


def solution(mesh):
    return jax.shard_map(
        local,
        mesh=mesh,
        in_specs=(P(("fs", "tp"), None), P(), P("fs", "tp"), P("fs", "tp"), P("tp", "fs")),
        out_specs=P(("fs", "tp"), None),
        check_vma=False,
    )
```

```python
import jax
import jax.numpy as jnp
from jax import lax
from jax.experimental import pallas as pl
from jax.experimental.pallas import tpu as pltpu
from jax.sharding import PartitionSpec as P

MESH = pl.DeviceIdType.MESH
BF, F32 = jnp.bfloat16, jnp.float32
eps_floor = 0.05

D, T, HU, HP = 2048, 128, 352, 384
GATE_A, UP_A, GATE_B, UP_B, DOWN_A, DOWN_B = range(6)
PAIRS = (((0, 0), (0, 1)), ((1, 0), (-1, 0)), ((1, 1), (0, -1)), ((1, -1), (-1, 1)), ((0, 2), (-1, -1)), ((2, 0), (1, 2)), ((2, 1), (-1, 2)), ((2, -1), (2, 2)))
W, S, C = 0, 1, 2
EVENTS = (
    (C, "own", 0), (C, "own", 1), (C, "own", 4), (S, 0, 0, 0, 0, 1), (S, 0, 0, 0, 0, -1), (S, 0, 0, 0, 1, 1),
    (S, 0, 0, 0, 1, -1), (C, "tokens_out"), (S, 1, 0, 0, 1, 1), (S, 1, 0, 0, 1, -1), (S, 1, 0, 0, 0, 1),
    (S, 1, 0, 0, 0, -1), (S, 4, 0, 0, 0, -1), (W, 0, 0, -1), (W, 0, 0, 1), (W, 0, -1, 0), (W, 0, 1, 0),
    (S, 0, 0, -1, 0, 1), (S, 0, 0, -1, 0, -1), (S, 0, 0, -1, 1, 1), (S, 0, 0, 1, 0, 1), (S, 0, 0, 1, 0, -1),
    (C, "normalize", 0), (W, 1, -1, 0), (W, 1, 1, 0), (W, 1, 0, -1), (W, 1, 0, 1), (S, 1, -1, 0, 0, 1),
    (S, 1, 0, -1, 0, -1), (S, 0, -1, 0, 0, 1), (S, 4, 0, 0, 1, -1), (S, 1, 0, -1, 0, 1), (S, 1, 0, 1, 0, -1),
    (W, 0, -1, -1), (W, 0, -1, 1), (W, 0, 2, 0), (W, 4, 0, 1), (S, 1, 0, -1, 1, 1), (S, 1, 0, 1, 0, 1),
    (S, 0, 2, 0, 1, -1), (W, 0, 1, -1), (W, 0, 1, 1), (W, 1, 0, 2), (W, 1, -1, 1), (C, "plane_b", 0), (C, "own", 2),
    (C, "plane_b", 1), (C, "own", 3), (S, 2, 0, 0, 0, -1), (S, 2, 0, 0, 0, 1), (S, 0, -1, -1, 1, 1),
    (S, 2, 0, 0, 1, -1), (S, 3, 0, 0, 1, -1), (W, 0, 0, 2), (W, 4, 1, 0), (W, 1, -1, -1), (W, 1, 1, 1),
    (S, 1, -1, -1, 1, 1), (S, 0, 2, 0, 1, 1), (S, 3, 0, 0, 0, -1), (W, 1, 2, 0), (S, 1, 2, 0, 1, -1), (W, 1, 1, -1),
    (W, 0, 1, 2), (S, 1, 2, 0, 1, 1), (W, 2, 0, 1), (S, 0, 1, -1, 1, 1), (S, 4, 0, 1, 0, -1), (W, 2, 0, -1),
    (S, 2, 0, 1, 0, -1), (W, 0, 2, -1), (W, 2, 1, 0), (S, 1, 1, -1, 1, 1), (W, 3, 1, 0), (S, 2, 0, 0, 1, 1),
    (W, 1, 2, -1), (S, 2, 0, -1, 0, -1), (W, 0, -1, 2), (W, 3, 0, 1), (S, 3, 0, 1, 0, -1), (S, 0, -1, 2, 0, 1),
    (W, 1, 1, 2), (C, "down_out"), (W, 1, -1, 2), (S, 1, -1, 2, 0, 1), (S, 3, 0, 0, 1, 1), (S, 3, 0, 0, 0, 1),
    (W, 0, 2, 1), (W, 4, 1, 1), (W, 2, 1, 1), (S, 2, 0, 1, 0, 1), (S, 2, 0, -1, 1, 1), (C, "tokens_on"),
    (W, 1, 2, 1), (C, "normalize", 1), (S, 2, 0, -1, 0, 1), (S, 3, 0, 1, 0, 1), (W, 2, -1, 0), (W, 3, 1, 1),
    (W, 2, -1, 1), (C, "tokens_in", 2), (C, "normalize", 2), (S, 2, -1, 0, 0, 1), (W, 0, 2, 2), (W, 1, 2, 2),
    (W, 3, -1, 0), (W, 3, 0, -1), (S, 3, 0, -1, 0, -1), (S, 3, -1, 0, 0, 1), (S, 3, 0, -1, 1, 1), (W, 2, 1, -1),
    (W, 2, 2, 0), (S, 2, 2, 0, 1, -1), (S, 3, 0, -1, 0, 1), (S, 4, 0, 0, 1, 1), (W, 2, -1, -1), (W, 3, 1, -1),
    (S, 3, 1, -1, 1, 1), (S, 2, 1, -1, 1, 1), (W, 2, 0, 2), (W, 3, -1, 1), (S, 2, 2, 0, 1, 1), (W, 3, 2, 0),
    (S, 3, 2, 0, 1, -1), (S, 3, 2, 0, 1, 1), (W, 3, 0, 2), (W, 3, 2, 1), (C, "plane_b", 2), (C, "own", 5),
    (S, 5, 0, 0, 1, -1), (S, 5, 0, 0, 0, -1), (W, 2, 1, 2), (S, 2, -1, -1, 1, 1), (W, 3, -1, -1),
    (S, 3, -1, -1, 1, 1), (W, 4, -1, 0), (C, "tokens_in", 3), (C, "normalize", 3), (S, 5, 0, 0, 0, 1), (W, 2, 2, 1),
    (C, "matmul", True, 0, 0), (W, 3, 1, 2), (S, 4, 0, 0, 0, 1), (W, 3, -1, 2), (S, 3, -1, 2, 0, 1),
    (C, "matmul", True, 0, 1), (W, 2, -1, 2), (S, 2, -1, 2, 0, 1), (S, 4, 0, 1, 0, 1), (W, 5, 1, 0),
    (C, "matmul", True, 0, 2), (W, 5, 0, 1), (S, 5, 0, 1, 0, -1), (S, 5, 0, 1, 0, 1), (C, "gating", True, 0),
    (S, 5, 0, 0, 1, 1), (W, 3, 2, -1), (W, 2, 2, -1), (C, "from_sibling", 0), (C, "matmul", False, 0, 0),
    (W, 5, 0, -1), (W, 3, 2, 2), (S, 5, 0, -1, 0, -1), (S, 4, -1, 0, 0, 1), (S, 5, 0, -1, 0, 1),
    (C, "matmul", False, 0, 1), (C, "matmul", False, 0, 2), (W, 4, 0, -1), (S, 4, 0, -1, 0, -1), (W, 2, 2, 2),
    (C, "gating", False, 0), (S, 4, 0, -1, 1, 1), (S, 5, 0, -1, 1, 1), (W, 4, 1, -1), (C, "matmul", True, 1, 0),
    (W, 5, 1, 1), (S, 4, 1, -1, 1, 1), (S, 4, 0, -1, 0, 1), (C, "matmul", True, 1, 1), (W, 5, -1, 0), (W, 5, 1, -1),
    (C, "matmul", True, 1, 2), (S, 5, -1, 0, 0, 1), (S, 5, 1, -1, 1, 1), (C, "gating", True, 1), (W, 5, -1, 1),
    (W, 4, -1, 1), (W, 5, -1, -1), (W, 4, 0, 2), (S, 5, -1, -1, 1, 1), (C, "from_sibling", 1),
    (C, "matmul", False, 1, 0), (C, "matmul", False, 1, 1), (W, 4, 2, 0), (S, 4, 2, 0, 1, -1), (S, 4, 2, 0, 1, 1),
    (W, 5, 2, 0), (S, 5, 2, 0, 1, -1), (C, "matmul", False, 1, 2), (S, 5, 2, 0, 1, 1), (W, 4, 2, 1), (W, 4, -1, -1),
    (S, 4, -1, -1, 1, 1), (C, "gating", False, 1), (C, "down_pair", 0), (W, 5, 0, 2), (W, 5, 2, 1), (W, 4, 1, 2),
    (W, 5, 1, 2), (C, "down_pair", 1), (W, 4, -1, 2), (S, 4, -1, 2, 0, 1), (W, 5, 2, -1), (W, 4, 2, -1),
    (W, 5, -1, 2), (S, 5, -1, 2, 0, 1), (C, "down_pair", 2), (W, 4, 2, 2), (C, "relay", 0), (W, 5, 2, 2),
    (C, "down_pair", 3), (C, "relay", 1), (C, "down_pair", 4), (C, "relay", 2), (C, "finish", 0),
    (C, "down_pair", 5), (C, "relay", 3), (C, "finish", 1), (C, "down_pair", 6), (C, "relay", 4), (C, "finish", 2),
    (C, "down_pair", 7), (C, "relay", 5), (C, "finish", 3), (C, "relay", 6), (C, "finish", 4), (C, "relay", 7),
    (C, "finish", 5), (C, "finish", 6), (C, "finish", 7),
)


def kernel(tok, gain, gate, up, down, out, wg, wd, x4, nrm, acc, hid, pb, rb, qb, mid, own, ob,
           in_sem, ssem, rsem, dsend, drecv_g, drecv_d, zsend, zrecv, tsend, trecv, psend, precv, osem):
    fs, tp = lax.axis_index("fs"), lax.axis_index("tp")
    y, x, z, c = fs // 4, fs % 4, tp // 2, tp % 2
    d = 1 - 2 * c
    par = (x + y) % 2
    pars = (par, 1 - par, par, 1 - par, 1 - par, par)
    sibling = (fs, z * 2 + 1 - c)

    def zdev(k):
        return (fs, ((z + k * d + 8) % 8) * 2 + c)

    def fpos(t, i, j):
        p = pars[t]
        yy = (y + d * (i * p + j * (1 - p)) + 8) % 4
        xx = (x + d * (i * (1 - p) + j * p) + 8) % 4
        return yy * 4 + xx

    def piece(t, core, f):
        if t < 4:
            return wg.at[core, t // 2, f, t % 2, pl.ds(0, HU), :]
        return wd.at[f, core * 2 + (t - 4), pl.ds(0, HU), :]

    def rcopy(src, dst, s, r, dev):
        return pltpu.make_async_remote_copy(
            src_ref=src, dst_ref=dst, send_sem=s, recv_sem=r, device_id=dev, device_id_type=MESH
        )

    def send(t, i, j, axis, step):
        f = fpos(t, i, j)
        ref = piece(t, c, f)
        to = fpos(t, step, 0) if axis == 0 else fpos(t, 0, step)
        rcopy(ref, ref, ssem.at[t], rsem.at[t, f], (to, tp)).start()

    def across(t, i, j):
        f = fpos(t, i, j)
        ref = piece(t, c, f)
        r = drecv_g.at[t // 2] if t < 4 else drecv_d.at[t - 4, f]
        rcopy(ref, ref, dsend.at[t], r, sibling).start()

    def got(t, i, j):
        f = fpos(t, i, j)
        ref = piece(t, c, f)
        rcopy(ref, ref, ssem.at[t], rsem.at[t, f], sibling).wait_recv()

    def own_ready(t):
        across(t, 0, 0)

    def normalize(slot):
        def rows(i, _):
            at = pl.multiple_of(i * 16, 16)
            v = x4[slot, pl.ds(at, 16), :].astype(F32)
            factor = lax.rsqrt(jnp.sum(v * v, axis=-1, keepdims=True) * (1.0 / D) + eps_floor)
            nrm[pl.ds(pl.multiple_of(slot * T + at, 16), 16), :] = (v * factor * gain[...]).astype(BF)
            return 0

        lax.fori_loop(0, T // 16, rows, 0)

    def matmul(mine, ab, n):
        core = c if mine else 1 - c
        rows = [wg[core, ab, f, h, n * 128 : (n + 1) * 128, :] for h in (0, 1) for f in range(16)]
        w = jnp.concatenate([jnp.concatenate(rows[:16], axis=1), jnp.concatenate(rows[16:], axis=1)], axis=0)
        both = lax.dot_general(nrm[...], w, (((1,), (1,)), ((), ())), preferred_element_type=F32)
        acc[:, n * 256 : (n + 1) * 256] = both

    def gating(mine, ab):
        core = c if mine else 1 - c
        lanes = pl.ds(pl.multiple_of((core * 2 + ab) * HP, 128), HP)

        def rows(i, _):
            at = pl.ds(pl.multiple_of(i * 32, 32), 32)
            v = acc[at, :]
            g = jnp.concatenate([v[:, n * 256 : n * 256 + 128] for n in range(3)], axis=1)
            u = jnp.concatenate([v[:, n * 256 + 128 : n * 256 + 256] for n in range(3)], axis=1)
            hid[at, lanes] = (g / (1.0 + jnp.exp(-g)) * u).astype(BF)
            return 0

        lax.fori_loop(0, 16, rows, 0)

    def from_sibling(ab):
        every = wg.at[1 - c, ab, :, :, pl.ds(0, HU), :]
        rcopy(every, every, dsend.at[ab], drecv_g.at[ab], sibling).wait_recv()

    def pair_fs(p):
        return [fpos(DOWN_A, *o) for o in PAIRS[p]]

    def down_pair(p):
        fa, fb = pair_fs(p)
        for t in (DOWN_A, DOWN_B):
            for f in (fa, fb):
                ref = piece(t, 1 - c, f)
                rcopy(ref, ref, dsend.at[t], drecv_d.at[t - 4, f], sibling).wait_recv()
        w = jnp.concatenate([wd[fa].reshape(4 * HP, 128), wd[fb].reshape(4 * HP, 128)], axis=1)
        part = jnp.dot(hid[...], w, preferred_element_type=F32)
        for s in (3, 2):
            for h in (0, 1):
                pb[s - 1, p, h] = part[s * T : (s + 1) * T, h * 128 : (h + 1) * 128].astype(BF)
        own[p] = part[0:T]
        mid[p] = part[T : 2 * T]
        rcopy(pb.at[2, p], qb.at[p], psend.at[2], precv.at[2, p], zdev(-1)).start()
        rcopy(pb.at[1, p], rb.at[1, p], psend.at[1], precv.at[1, p], zdev(1)).start()

    def relay(p):
        rcopy(qb.at[p], qb.at[p], psend.at[2], precv.at[2, p], sibling).wait_recv()
        for h in (0, 1):
            pb[0, p, h] = (mid[p, :, h * 128 : (h + 1) * 128] + qb[p, h].astype(F32)).astype(BF)
        rcopy(pb.at[0, p], rb.at[0, p], psend.at[0], precv.at[0, p], zdev(-1)).start()

    def finish(p):
        for s in (0, 1):
            rcopy(rb.at[s, p], rb.at[s, p], psend.at[s], precv.at[s, p], sibling).wait_recv()
        for h, f in enumerate(pair_fs(p)):
            v = own[p, :, h * 128 : (h + 1) * 128]
            for s in (0, 1):
                v = v + rb[s, p, h].astype(F32)
            ob[p, h] = v.astype(BF)
            pltpu.make_async_copy(ob.at[p, h], out.at[:, pl.ds(pl.multiple_of(f * 128, 128), 128)], osem).start()

    inputs = [
        pltpu.make_async_copy(gate, piece(GATE_A, c, fs), in_sem.at[0]),
        pltpu.make_async_copy(up, piece(UP_A, c, fs), in_sem.at[1]),
        pltpu.make_async_copy(down, piece(DOWN_A, c, fs), in_sem.at[2]),
        pltpu.make_async_copy(tok, x4.at[0], in_sem.at[3]),
    ]
    for cp in inputs:
        cp.start()
    barrier = pltpu.get_barrier_semaphore()
    partners = [zdev(k) for k in (4, 1, -1)]
    partners += [(fpos(0, *o), tp) for o in ((1, 0), (-1, 0), (0, 1), (0, -1))] + [sibling]
    for dev in partners:
        pl.semaphore_signal(barrier, inc=1, device_id=dev, device_id_type=MESH)
    for f in range(16):
        for b in range(4):
            wd[f, b, HU:HP, :] = jnp.zeros((HP - HU, 128), BF)
            for h in (0, 1):
                wg[b // 2, b % 2, f, h, HU:HP, :] = jnp.zeros((HP - HU, 128), BF)
    for cp in inputs:
        cp.wait()
    pl.semaphore_wait(barrier, len(partners))

    gz = [rcopy(piece(t, c, fs), piece(t + 2, c, fs), zsend.at[t], zrecv.at[t], zdev(4)) for t in (GATE_A, UP_A)]
    dz = rcopy(piece(DOWN_A, c, fs), piece(DOWN_B, c, fs), zsend.at[2], zrecv.at[2], zdev(4))
    t2 = rcopy(x4.at[0], x4.at[2], tsend, trecv.at[2], zdev(-1))
    t1 = rcopy(x4.at[0], x4.at[1], tsend, trecv.at[1], zdev(1))
    t3 = rcopy(x4.at[1], x4.at[3], tsend, trecv.at[3], zdev(1))

    def plane_b(k):
        (gz[0], gz[1], dz)[k].wait_recv()

    def tokens_out():
        for cp in (gz[0], gz[1], t2, t1):
            cp.start()

    def tokens_on():
        t1.wait_recv()
        t3.start()

    def down_out():
        dz.start()

    def tokens_in(k):
        (None, None, t2, t3)[k].wait_recv()

    tasks = {
        "own": own_ready, "plane_b": plane_b, "tokens_out": tokens_out, "tokens_on": tokens_on,
        "down_out": down_out, "tokens_in": tokens_in, "normalize": normalize, "from_sibling": from_sibling,
        "matmul": matmul, "gating": gating, "down_pair": down_pair, "relay": relay, "finish": finish,
    }

    def event(kind, *rest):
        if kind == W:
            got(*rest)
            across(*rest)
        elif kind == S:
            send(*rest)
        else:
            tasks[rest[0]](*rest[1:])

    for e in EVENTS:
        event(*e)

    for t in range(6):
        if t < 4:
            few = wg.at[c, t // 2, pl.ds(0, 15), t % 2, pl.ds(0, HU), :]
            all16 = wg.at[c, t // 2, :, t % 2, pl.ds(0, HU), :]
        else:
            few = wd.at[pl.ds(0, 15), 0, pl.ds(0, HU), :]
            all16 = wd.at[:, 0, pl.ds(0, HU), :]
        rcopy(few, few, ssem.at[t], rsem.at[t, 0], sibling).wait_send()
        rcopy(all16, all16, dsend.at[t], rsem.at[t, 0], sibling).wait_send()
    for cp in (*gz, dz):
        cp.wait_send()
    three = x4.at[pl.ds(0, 3)]
    rcopy(three, three, tsend, trecv.at[1], sibling).wait_send()
    for s in range(3):
        rcopy(pb.at[s], pb.at[s], psend.at[s], precv.at[s, 0], sibling).wait_send()
    pltpu.make_async_copy(x4.at[0], out, osem).wait()


def local(tokens, norm_gain, gate_weight, up_weight, down_weight):
    hbm = pl.BlockSpec(memory_space=pl.ANY)
    vmem = pl.BlockSpec(memory_space=pltpu.VMEM)
    dma = pltpu.SemaphoreType.DMA
    return pl.pallas_call(
        kernel,
        out_shape=jax.ShapeDtypeStruct((T, D), BF),
        in_specs=[hbm, vmem, hbm, hbm, hbm],
        out_specs=hbm,
        scratch_shapes=[
            pltpu.VMEM((2, 2, 16, 2, HP, 128), BF),
            pltpu.VMEM((16, 4, HP, 128), BF),
            pltpu.VMEM((4, T, D), BF),
            pltpu.VMEM((4 * T, D), BF),
            pltpu.VMEM((4 * T, 2 * HP), F32),
            pltpu.VMEM((4 * T, 4 * HP), BF),
            pltpu.VMEM((3, 8, 2, T, 128), BF),
            pltpu.VMEM((2, 8, 2, T, 128), BF),
            pltpu.VMEM((8, 2, T, 128), BF),
            pltpu.VMEM((8, T, 256), F32),
            pltpu.VMEM((8, T, 256), F32),
            pltpu.VMEM((8, 2, T, 128), BF),
            dma((4,)),
            dma((6,)),
            dma((6, 16)),
            dma((6,)),
            dma((2,)),
            dma((2, 16)),
            dma((3,)),
            dma((3,)),
            dma(()),
            dma((4,)),
            dma((3,)),
            dma((3, 8)),
            dma(()),
        ],
        compiler_params=pltpu.CompilerParams(
            collective_id=0, has_side_effects=True, vmem_limit_bytes=58 * 2**20
        ),
    )(tokens, norm_gain.reshape(1, D), gate_weight.T, up_weight.T, down_weight)


def solution(mesh):
    return jax.shard_map(
        local,
        mesh=mesh,
        in_specs=(P(("fs", "tp"), None), P(), P("fs", "tp"), P("fs", "tp"), P("tp", "fs")),
        out_specs=P(("fs", "tp"), None),
        check_vma=False,
    )
```

```python
import jax
import jax.numpy as jnp
from jax import lax
from jax.experimental import pallas as pl
from jax.experimental.pallas import tpu as pltpu
from jax.sharding import PartitionSpec as P

MESH = pl.DeviceIdType.MESH
BF, F32 = jnp.bfloat16, jnp.float32
eps_floor = 0.05

D, T, HU, HP = 2048, 128, 352, 384
GATE_A, UP_A, GATE_B, UP_B, DOWN_A, DOWN_B = range(6)
PAIRS = (((0, 0), (-1, 0)), ((1, 0), (0, -1)), ((0, 1), (0, 2)), ((-1, 1), (1, -1)), ((-1, -1), (1, 1)), ((2, -1), (2, 1)), ((2, 0), (-1, 2)), ((1, 2), (2, 2)))
W, S, C = 0, 1, 2
EVENTS = (
    (C, "own", 0), (C, "own", 1), (C, "own", 4), (S, 0, 0, 0, 0, 1), (S, 0, 0, 0, 0, -1), (S, 0, 0, 0, 1, 1),
    (S, 0, 0, 0, 1, -1), (S, 1, 0, 0, 1, 1), (S, 1, 0, 0, 1, -1), (S, 1, 0, 0, 0, 1), (S, 1, 0, 0, 0, -1),
    (C, "tokens_out", 0), (S, 4, 0, 0, 0, -1), (W, 0, 0, -1), (W, 0, 0, 1), (W, 0, -1, 0), (W, 0, 1, 0),
    (S, 0, 0, -1, 0, 1), (S, 0, 0, -1, 0, -1), (S, 0, 0, -1, 1, 1), (S, 0, 0, 1, 0, 1), (S, 0, 0, 1, 0, -1),
    (S, 0, -1, 0, 0, 1), (C, "normalize", 0), (S, 4, 0, 0, 1, -1), (W, 1, -1, 0), (W, 1, 1, 0), (W, 1, 0, -1),
    (W, 1, 0, 1), (S, 1, -1, 0, 0, 1), (S, 1, 0, -1, 0, -1), (S, 1, 0, -1, 0, 1), (S, 1, 0, 1, 0, -1),
    (S, 1, 0, -1, 1, 1), (S, 1, 0, 1, 0, 1), (W, 0, -1, -1), (W, 0, -1, 1), (W, 0, 2, 0), (W, 4, 0, 1),
    (S, 0, 2, 0, 1, -1), (S, 0, -1, -1, 1, 1), (S, 0, 2, 0, 1, 1), (W, 0, 1, -1), (W, 0, 1, 1), (W, 1, 0, 2),
    (W, 1, -1, 1), (S, 0, 1, -1, 1, 1), (C, "plane_b", 0), (C, "own", 2), (C, "plane_b", 1), (C, "own", 3),
    (S, 2, 0, 0, 0, -1), (S, 2, 0, 0, 0, 1), (S, 2, 0, 0, 1, -1), (S, 3, 0, 0, 1, -1), (S, 3, 0, 0, 0, -1),
    (S, 2, 0, 0, 1, 1), (S, 3, 0, 0, 1, 1), (S, 3, 0, 0, 0, 1), (C, "tokens_out", 1), (W, 0, 0, 2), (W, 4, 1, 0),
    (W, 1, -1, -1), (W, 1, 1, 1), (S, 1, -1, -1, 1, 1), (W, 1, 2, 0), (S, 1, 2, 0, 1, -1), (S, 1, 2, 0, 1, 1),
    (S, 4, 0, 1, 0, -1), (W, 1, 1, -1), (W, 0, 1, 2), (S, 1, 1, -1, 1, 1), (W, 2, 0, 1), (S, 2, 0, 1, 0, -1),
    (S, 2, 0, 1, 0, 1), (W, 2, 0, -1), (S, 2, 0, -1, 0, -1), (S, 2, 0, -1, 1, 1), (S, 2, 0, -1, 0, 1),
    (W, 0, 2, -1), (W, 2, 1, 0), (C, "tokens_on"), (W, 3, 1, 0), (W, 1, 2, -1), (C, "normalize", 1), (W, 0, -1, 2),
    (W, 3, 0, 1), (S, 3, 0, 1, 0, -1), (S, 0, -1, 2, 0, 1), (S, 3, 0, 1, 0, 1), (W, 1, 1, 2), (W, 1, -1, 2),
    (S, 1, -1, 2, 0, 1), (W, 0, 2, 1), (W, 4, 1, 1), (W, 2, 1, 1), (W, 1, 2, 1), (W, 2, -1, 0), (W, 3, 1, 1),
    (S, 2, -1, 0, 0, 1), (W, 2, -1, 1), (W, 0, 2, 2), (W, 1, 2, 2), (C, "down_out"), (W, 3, -1, 0), (W, 3, 0, -1),
    (S, 3, 0, -1, 0, -1), (S, 3, -1, 0, 0, 1), (S, 3, 0, -1, 1, 1), (S, 3, 0, -1, 0, 1), (S, 4, 0, 0, 1, 1),
    (W, 2, 1, -1), (W, 2, 2, 0), (S, 2, 2, 0, 1, -1), (S, 2, 1, -1, 1, 1), (S, 2, 2, 0, 1, 1), (W, 2, -1, -1),
    (S, 2, -1, -1, 1, 1), (W, 3, 1, -1), (S, 3, 1, -1, 1, 1), (W, 2, 0, 2), (W, 3, -1, 1), (W, 3, 2, 0),
    (S, 3, 2, 0, 1, -1), (S, 3, 2, 0, 1, 1), (W, 3, 0, 2), (S, 4, 0, 0, 0, 1), (C, "tokens_in", 2),
    (C, "normalize", 2), (W, 3, 2, 1), (C, "tokens_in", 3), (C, "normalize", 3), (W, 2, 1, 2), (W, 3, -1, -1),
    (S, 3, -1, -1, 1, 1), (W, 4, -1, 0), (S, 4, 0, 1, 0, 1),
)
GATE_EVENTS = {
    1: (
        (W, 2, 2, 1),
    ),
    2: (
        (S, 4, -1, 0, 0, 1), (W, 3, 1, 2), (W, 3, -1, 2), (W, 2, -1, 2), (S, 2, -1, 2, 0, 1), (S, 3, -1, 2, 0, 1),
    ),
    4: (
        (W, 3, 2, -1), (W, 2, 2, -1), (C, "from_sibling", 0),
    ),
    5: (
        (W, 4, 0, -1), (S, 4, 0, -1, 1, 1), (S, 4, 0, -1, 0, -1), (S, 4, 0, -1, 0, 1),
    ),
    6: (
        (C, "plane_b", 2), (C, "own", 5), (S, 5, 0, 0, 0, -1), (S, 5, 0, 0, 0, 1), (S, 5, 0, 0, 1, -1),
    ),
    7: (
        (W, 2, 2, 2), (W, 3, 2, 2), (S, 5, 0, 0, 1, 1),
    ),
    8: (
        (W, 4, 1, -1), (S, 4, 1, -1, 1, 1),
    ),
    10: (
        (W, 4, 2, 0), (S, 4, 2, 0, 1, -1), (S, 4, 2, 0, 1, 1),
    ),
    11: (
        (W, 4, -1, 1), (W, 4, 0, 2), (W, 5, 0, 1), (S, 5, 0, 1, 0, -1), (S, 5, 0, 1, 0, 1),
    ),
    12: (
        (W, 5, 0, -1), (S, 5, 0, -1, 1, 1), (C, "from_sibling", 1),
    ),
    13: (
        (S, 5, 0, -1, 0, -1), (S, 5, 0, -1, 0, 1),
    ),
    14: (
        (W, 5, 1, 0), (W, 4, -1, -1), (W, 4, 2, 1),
    ),
    15: (
        (W, 5, -1, 0),
    ),
}
DOWN_EVENTS = {
    0: (
        (S, 4, -1, -1, 1, 1), (W, 4, 1, 2),
    ),
    1: (
        (W, 5, 2, 0), (S, 5, 2, 0, 1, 1), (S, 5, 2, 0, 1, -1), (W, 4, -1, 2), (S, 4, -1, 2, 0, 1),
        (S, 5, -1, 0, 0, 1), (W, 5, 1, 1),
    ),
    2: (
        (W, 5, 1, -1), (S, 5, 1, -1, 1, 1), (W, 5, -1, 1), (W, 5, -1, -1), (W, 5, -1, 2), (W, 5, 1, 2),
        (S, 5, -1, 2, 0, 1), (S, 5, -1, -1, 1, 1),
    ),
    3: (
        (W, 4, 2, -1), (W, 4, 2, 2), (W, 5, 0, 2), (W, 5, 2, 1),
    ),
    4: (
        (W, 5, 2, 2), (W, 5, 2, -1),
    ),
    9: (
        (C, "drain", 0), (C, "drain", 1), (C, "drain", 2), (C, "drain", 3), (C, "drain", 6),
    ),
    10: (
        (C, "drain", 4), (C, "drain", 5),
    ),
}
LAG = 2


def kernel(tok, gain, gate, up, down, out, wg, wd, x4, nrm, acc, hid, pb, rb, qb, mid, own, ob,
           in_sem, ssem, rsem, dsend, drecv_g, drecv_d, zsend, zrecv, tsend, trecv, psend, precv, osem):
    fs, tp = lax.axis_index("fs"), lax.axis_index("tp")
    y, x, z, c = fs // 4, fs % 4, tp // 2, tp % 2
    d = 1 - 2 * c
    par = (x + y) % 2
    pars = (par, 1 - par, par, 1 - par, 1 - par, par)
    sibling = (fs, z * 2 + 1 - c)

    def zdev(k):
        return (fs, ((z + k * d + 8) % 8) * 2 + c)

    def fpos(t, i, j):
        p = pars[t]
        yy = (y + d * (i * p + j * (1 - p)) + 8) % 4
        xx = (x + d * (i * (1 - p) + j * p) + 8) % 4
        return yy * 4 + xx

    def piece(t, core, f):
        if t < 4:
            return wg.at[core, t // 2, f, t % 2, pl.ds(0, HU), :]
        return wd.at[f, core * 2 + (t - 4), pl.ds(0, HU), :]

    def rcopy(src, dst, s, r, dev):
        return pltpu.make_async_remote_copy(
            src_ref=src, dst_ref=dst, send_sem=s, recv_sem=r, device_id=dev, device_id_type=MESH
        )

    def send(t, i, j, axis, step):
        f = fpos(t, i, j)
        ref = piece(t, c, f)
        to = fpos(t, step, 0) if axis == 0 else fpos(t, 0, step)
        rcopy(ref, ref, ssem.at[t], rsem.at[t, f], (to, tp)).start()

    def across(t, i, j):
        f = fpos(t, i, j)
        ref = piece(t, c, f)
        r = drecv_g.at[t // 2] if t < 4 else drecv_d.at[t - 4, f]
        rcopy(ref, ref, dsend.at[t], r, sibling).start()

    def got(t, i, j):
        f = fpos(t, i, j)
        ref = piece(t, c, f)
        rcopy(ref, ref, ssem.at[t], rsem.at[t, f], sibling).wait_recv()

    def own_ready(t):
        across(t, 0, 0)

    def normalize(slot):
        def rows(i, _):
            at = pl.multiple_of(i * 16, 16)
            v = x4[slot, pl.ds(at, 16), :].astype(F32)
            factor = lax.rsqrt(jnp.sum(v * v, axis=-1, keepdims=True) * (1.0 / D) + eps_floor)
            nrm[pl.ds(pl.multiple_of(slot * T + at, 16), 16), :] = (v * factor * gain[...]).astype(BF)
            return 0

        lax.fori_loop(0, T // 16, rows, 0)

    def block_of(b):
        return (1 - c if b % 2 else c), b // 2

    def matmul(b):
        core, ab = block_of(b)

        def columns(n, _):
            events_at({m: GATE_EVENTS[4 * b + m] for m in (1, 2) if 4 * b + m in GATE_EVENTS}, n)
            at = pl.ds(pl.multiple_of(n * 128, 128), 128)
            rows = [wg[core, ab, f, h, at, :] for h in (0, 1) for f in range(16)]
            w = jnp.concatenate([jnp.concatenate(rows[:16], axis=1), jnp.concatenate(rows[16:], axis=1)], axis=0)
            both = lax.dot_general(nrm[...], w, (((1,), (1,)), ((), ())), preferred_element_type=F32)
            acc[:, pl.ds(pl.multiple_of(n * 256, 256), 256)] = both
            return 0

        lax.fori_loop(0, 3, columns, 0)

    def gating(b):
        core, ab = block_of(b)
        lanes = pl.ds(pl.multiple_of((core * 2 + ab) * HP, 128), HP)

        def rows(i, _):
            at = pl.ds(pl.multiple_of(i * 32, 32), 32)
            v = acc[at, :]
            g = jnp.concatenate([v[:, n * 256 : n * 256 + 128] for n in range(3)], axis=1)
            u = jnp.concatenate([v[:, n * 256 + 128 : n * 256 + 256] for n in range(3)], axis=1)
            hid[at, lanes] = (g / (1.0 + jnp.exp(-g)) * u).astype(BF)
            return 0

        lax.fori_loop(0, 16, rows, 0)

    def from_sibling(ab):
        every = wg.at[1 - c, ab, :, :, pl.ds(0, HU), :]
        rcopy(every, every, dsend.at[ab], drecv_g.at[ab], sibling).wait_recv()

    def pair_fs(p):
        picked = []
        for h in (0, 1):
            i, j = PAIRS[0][h]
            for k in range(1, 8):
                i = jnp.where(p == k, PAIRS[k][h][0], i)
                j = jnp.where(p == k, PAIRS[k][h][1], j)
            picked.append(fpos(DOWN_A, i, j))
        return picked

    def down_pair(p):
        fa, fb = pair_fs(p)
        for t in (DOWN_A, DOWN_B):
            for f in (fa, fb):
                ref = piece(t, 1 - c, f)
                rcopy(ref, ref, dsend.at[t], drecv_d.at[t - 4, f], sibling).wait_recv()
        w = jnp.concatenate([wd[fa].reshape(4 * HP, 128), wd[fb].reshape(4 * HP, 128)], axis=1)
        part = jnp.dot(hid[...], w, preferred_element_type=F32)
        for s in (3, 2):
            for h in (0, 1):
                pb[s - 1, p, h] = part[s * T : (s + 1) * T, h * 128 : (h + 1) * 128].astype(BF)
        own[p] = part[0:T]
        mid[p] = part[T : 2 * T]
        rcopy(pb.at[2, p], qb.at[p], psend.at[2], precv.at[2, p], zdev(-1)).start()
        rcopy(pb.at[1, p], rb.at[1, p], psend.at[1], precv.at[1, p], zdev(1)).start()

    def relay(p):
        rcopy(qb.at[p], qb.at[p], psend.at[2], precv.at[2, p], sibling).wait_recv()
        for h in (0, 1):
            pb[0, p, h] = (mid[p, :, h * 128 : (h + 1) * 128] + qb[p, h].astype(F32)).astype(BF)
        rcopy(pb.at[0, p], rb.at[0, p], psend.at[0], precv.at[0, p], zdev(-1)).start()

    def finish(p):
        for s in (0, 1):
            rcopy(rb.at[s, p], rb.at[s, p], psend.at[s], precv.at[s, p], sibling).wait_recv()
        for h, f in enumerate(pair_fs(p)):
            v = own[p, :, h * 128 : (h + 1) * 128]
            for s in (0, 1):
                v = v + rb[s, p, h].astype(F32)
            ob[p, h] = v.astype(BF)
            pltpu.make_async_copy(ob.at[p, h], out.at[:, pl.ds(pl.multiple_of(f * 128, 128), 128)], osem).start()

    inputs = [
        pltpu.make_async_copy(gate, piece(GATE_A, c, fs), in_sem.at[0]),
        pltpu.make_async_copy(up, piece(UP_A, c, fs), in_sem.at[1]),
        pltpu.make_async_copy(down, piece(DOWN_A, c, fs), in_sem.at[2]),
        pltpu.make_async_copy(tok, x4.at[0], in_sem.at[3]),
    ]
    for cp in inputs:
        cp.start()
    barrier = pltpu.get_barrier_semaphore()
    partners = [zdev(k) for k in (4, 1, -1)]
    partners += [(fpos(0, *o), tp) for o in ((1, 0), (-1, 0), (0, 1), (0, -1))] + [sibling]
    for dev in partners:
        pl.semaphore_signal(barrier, inc=1, device_id=dev, device_id_type=MESH)
    for f in range(16):
        for b in range(4):
            wd[f, b, HU:HP, :] = jnp.zeros((HP - HU, 128), BF)
            for h in (0, 1):
                wg[b // 2, b % 2, f, h, HU:HP, :] = jnp.zeros((HP - HU, 128), BF)
    for cp in inputs:
        cp.wait()
    pl.semaphore_wait(barrier, len(partners))

    gz = [rcopy(piece(t, c, fs), piece(t + 2, c, fs), zsend.at[t], zrecv.at[t], zdev(4)) for t in (GATE_A, UP_A)]
    dz = rcopy(piece(DOWN_A, c, fs), piece(DOWN_B, c, fs), zsend.at[2], zrecv.at[2], zdev(4))
    t2 = rcopy(x4.at[0], x4.at[2], tsend, trecv.at[2], zdev(-1))
    t1 = rcopy(x4.at[0], x4.at[1], tsend, trecv.at[1], zdev(1))
    t3 = rcopy(x4.at[1], x4.at[3], tsend, trecv.at[3], zdev(1))

    def plane_b(k):
        (gz[0], gz[1], dz)[k].wait_recv()

    def tokens_out(k):
        for cp in ((gz[0], gz[1], t1), (t2,))[k]:
            cp.start()

    def tokens_on():
        t1.wait_recv()
        t3.start()

    def down_out():
        dz.start()

    def tokens_in(k):
        (None, None, t2, t3)[k].wait_recv()

    def drain(t):
        if t < 4:
            few = wg.at[c, t // 2, pl.ds(0, 15), t % 2, pl.ds(0, HU), :]
            all16 = wg.at[c, t // 2, :, t % 2, pl.ds(0, HU), :]
        elif t < 6:
            few = wd.at[pl.ds(0, 15), 0, pl.ds(0, HU), :]
            all16 = wd.at[:, 0, pl.ds(0, HU), :]
        else:
            for cp in (*gz, dz):
                cp.wait_send()
            three = x4.at[pl.ds(0, 3)]
            rcopy(three, three, tsend, trecv.at[1], sibling).wait_send()
            return
        rcopy(few, few, ssem.at[t], rsem.at[t, 0], sibling).wait_send()
        rcopy(all16, all16, dsend.at[t], rsem.at[t, 0], sibling).wait_send()

    tasks = {
        "own": own_ready, "plane_b": plane_b, "tokens_out": tokens_out, "tokens_on": tokens_on,
        "down_out": down_out, "tokens_in": tokens_in, "normalize": normalize, "from_sibling": from_sibling, "drain": drain,
    }

    def event(kind, *rest):
        if kind == W:
            got(*rest)
            across(*rest)
        elif kind == S:
            send(*rest)
        else:
            tasks[rest[0]](*rest[1:])

    def events_at(table, k):
        for at, some in table.items():

            @pl.when(k == at)
            def _():
                for e in some:
                    event(*e)

    for e in EVENTS:
        event(*e)

    for b in range(4):
        for e in GATE_EVENTS.get(4 * b, ()):
            event(*e)
        matmul(b)
        for e in GATE_EVENTS.get(4 * b + 3, ()):
            event(*e)
        gating(b)

    def down_step(k, _):
        events_at(DOWN_EVENTS, k)

        @pl.when(k < 8)
        def _():
            down_pair(k)

        @pl.when((k >= LAG) & (k < 8 + LAG))
        def _():
            relay(k - LAG)

        @pl.when(k >= 2 * LAG)
        def _():
            finish(k - 2 * LAG)

        return 0

    lax.fori_loop(0, 8 + 2 * LAG, down_step, 0)

    for s in range(3):
        rcopy(pb.at[s], pb.at[s], psend.at[s], precv.at[s, 0], sibling).wait_send()
    pltpu.make_async_copy(x4.at[0], out, osem).wait()


def local(tokens, norm_gain, gate_weight, up_weight, down_weight):
    hbm = pl.BlockSpec(memory_space=pl.ANY)
    vmem = pl.BlockSpec(memory_space=pltpu.VMEM)
    dma = pltpu.SemaphoreType.DMA
    return pl.pallas_call(
        kernel,
        out_shape=jax.ShapeDtypeStruct((T, D), BF),
        in_specs=[hbm, vmem, hbm, hbm, hbm],
        out_specs=hbm,
        scratch_shapes=[
            pltpu.VMEM((2, 2, 16, 2, HP, 128), BF),
            pltpu.VMEM((16, 4, HP, 128), BF),
            pltpu.VMEM((4, T, D), BF),
            pltpu.VMEM((4 * T, D), BF),
            pltpu.VMEM((4 * T, 2 * HP), F32),
            pltpu.VMEM((4 * T, 4 * HP), BF),
            pltpu.VMEM((3, 8, 2, T, 128), BF),
            pltpu.VMEM((2, 8, 2, T, 128), BF),
            pltpu.VMEM((8, 2, T, 128), BF),
            pltpu.VMEM((8, T, 256), F32),
            pltpu.VMEM((8, T, 256), F32),
            pltpu.VMEM((8, 2, T, 128), BF),
            dma((4,)),
            dma((6,)),
            dma((6, 16)),
            dma((6,)),
            dma((2,)),
            dma((2, 16)),
            dma((3,)),
            dma((3,)),
            dma(()),
            dma((4,)),
            dma((3,)),
            dma((3, 8)),
            dma(()),
        ],
        compiler_params=pltpu.CompilerParams(
            collective_id=0, has_side_effects=True, vmem_limit_bytes=58 * 2**20
        ),
    )(tokens, norm_gain.reshape(1, D), gate_weight.T, up_weight.T, down_weight)


def solution(mesh):
    return jax.shard_map(
        local,
        mesh=mesh,
        in_specs=(P(("fs", "tp"), None), P(), P("fs", "tp"), P("fs", "tp"), P("tp", "fs")),
        out_specs=P(("fs", "tp"), None),
        check_vma=False,
    )
```

```python
import jax
import jax.numpy as jnp
from jax import lax
from jax.experimental import pallas as pl
from jax.experimental.pallas import tpu as pltpu
from jax.sharding import PartitionSpec as P

MESH = pl.DeviceIdType.MESH
BF, F32 = jnp.bfloat16, jnp.float32
eps_floor = 0.05

D, T, HU, HP = 2048, 128, 352, 384
GATE_A, UP_A, GATE_B, UP_B, DOWN_A, DOWN_B = range(6)
PAIRS = (((0, 0), (-1, 0)), ((1, 0), (0, -1)), ((0, 1), (0, 2)), ((-1, 1), (1, -1)), ((-1, -1), (1, 1)), ((2, -1), (2, 1)), ((2, 0), (-1, 2)), ((1, 2), (2, 2)))
W, S, C = 0, 1, 2
EVENTS = (
    (C, "own", 0), (C, "own", 1), (C, "own", 4), (S, 0, 0, 0, 0, 1), (S, 0, 0, 0, 0, -1), (S, 0, 0, 0, 1, 1),
    (S, 0, 0, 0, 1, -1), (S, 1, 0, 0, 1, 1), (S, 1, 0, 0, 1, -1), (S, 1, 0, 0, 0, 1), (S, 1, 0, 0, 0, -1),
    (S, 4, 0, 0, 0, -1), (C, "tokens_out", 0), (S, 4, 0, 0, 1, -1), (W, 0, 0, -1), (W, 0, 0, 1), (W, 0, -1, 0),
    (W, 0, 1, 0), (S, 0, 0, -1, 0, 1), (S, 0, 0, -1, 0, -1), (S, 0, 0, -1, 1, 1), (S, 0, 0, 1, 0, 1),
    (S, 0, 0, 1, 0, -1), (S, 0, -1, 0, 0, 1), (C, "normalize", 0), (W, 1, -1, 0), (W, 1, 1, 0), (W, 1, 0, -1),
    (W, 1, 0, 1), (S, 1, -1, 0, 0, 1), (S, 1, 0, -1, 0, -1), (S, 1, 0, -1, 0, 1), (S, 1, 0, 1, 0, -1),
    (S, 1, 0, -1, 1, 1), (S, 1, 0, 1, 0, 1), (W, 0, -1, -1), (W, 0, -1, 1), (W, 0, 2, 0), (W, 4, 0, 1),
    (S, 0, 2, 0, 1, -1), (S, 0, -1, -1, 1, 1), (S, 0, 2, 0, 1, 1), (W, 0, 1, -1), (W, 0, 1, 1), (W, 1, 0, 2),
    (W, 1, -1, 1), (S, 0, 1, -1, 1, 1), (S, 4, 0, 1, 0, -1), (C, "plane_b", 0), (C, "own", 2), (C, "plane_b", 1),
    (C, "own", 3), (S, 2, 0, 0, 0, -1), (S, 2, 0, 0, 0, 1), (S, 2, 0, 0, 1, -1), (S, 3, 0, 0, 1, -1),
    (S, 3, 0, 0, 0, -1), (S, 2, 0, 0, 1, 1), (S, 3, 0, 0, 1, 1), (S, 3, 0, 0, 0, 1), (C, "tokens_out", 1),
    (W, 0, 0, 2), (W, 4, 1, 0), (W, 1, -1, -1), (W, 1, 1, 1), (S, 1, -1, -1, 1, 1), (W, 1, 2, 0),
    (S, 1, 2, 0, 1, -1), (S, 1, 2, 0, 1, 1), (W, 1, 1, -1), (W, 0, 1, 2), (S, 1, 1, -1, 1, 1), (W, 2, 0, 1),
    (S, 2, 0, 1, 0, -1), (S, 2, 0, 1, 0, 1), (W, 2, 0, -1), (S, 2, 0, -1, 0, -1), (S, 2, 0, -1, 1, 1),
    (S, 2, 0, -1, 0, 1), (W, 0, 2, -1), (W, 2, 1, 0), (C, "tokens_on"), (W, 3, 1, 0), (W, 1, 2, -1),
    (C, "normalize", 1), (W, 0, -1, 2), (W, 3, 0, 1), (S, 3, 0, 1, 0, -1), (S, 0, -1, 2, 0, 1), (S, 3, 0, 1, 0, 1),
    (W, 1, 1, 2), (W, 1, -1, 2), (S, 1, -1, 2, 0, 1), (W, 0, 2, 1), (W, 4, 1, 1), (W, 2, 1, 1), (W, 1, 2, 1),
    (S, 4, 0, 0, 1, 1), (W, 2, -1, 0), (W, 3, 1, 1), (S, 2, -1, 0, 0, 1), (W, 2, -1, 1), (W, 0, 2, 2), (W, 1, 2, 2),
    (C, "down_out"), (W, 3, -1, 0), (W, 3, 0, -1), (S, 3, 0, -1, 0, -1), (S, 3, -1, 0, 0, 1), (S, 3, 0, -1, 1, 1),
    (S, 3, 0, -1, 0, 1), (W, 2, 1, -1), (W, 2, 2, 0), (S, 2, 2, 0, 1, -1), (S, 2, 1, -1, 1, 1), (S, 2, 2, 0, 1, 1),
    (S, 4, 0, 0, 0, 1), (W, 2, -1, -1), (S, 2, -1, -1, 1, 1), (W, 3, 1, -1), (S, 3, 1, -1, 1, 1), (W, 2, 0, 2),
    (S, 4, 0, 1, 0, 1), (W, 3, -1, 1), (W, 3, 2, 0), (S, 3, 2, 0, 1, -1), (S, 3, 2, 0, 1, 1), (W, 3, 0, 2),
    (C, "tokens_in", 2), (C, "normalize", 2), (W, 3, 2, 1), (C, "tokens_in", 3), (C, "normalize", 3), (W, 2, 1, 2),
    (W, 3, -1, -1), (S, 3, -1, -1, 1, 1), (W, 4, -1, 0), (S, 4, -1, 0, 0, 1),
)
GATE_EVENTS = {
    1: (
        (W, 2, 2, 1),
    ),
    2: (
        (W, 3, 1, 2), (W, 3, -1, 2), (W, 2, -1, 2), (S, 2, -1, 2, 0, 1), (S, 3, -1, 2, 0, 1),
    ),
    4: (
        (W, 3, 2, -1), (W, 2, 2, -1), (C, "from_sibling", 0),
    ),
    5: (
        (W, 4, 0, -1), (S, 4, 0, -1, 1, 1), (S, 4, 0, -1, 0, -1), (S, 4, 0, -1, 0, 1),
    ),
    6: (
        (C, "plane_b", 2), (C, "own", 5), (S, 5, 0, 0, 0, -1), (S, 5, 0, 0, 0, 1), (S, 5, 0, 0, 1, -1),
        (S, 5, 0, 0, 1, 1),
    ),
    7: (
        (W, 2, 2, 2), (W, 3, 2, 2),
    ),
    8: (
        (W, 4, 1, -1), (S, 4, 1, -1, 1, 1),
    ),
    10: (
        (W, 4, 2, 0), (S, 4, 2, 0, 1, -1), (S, 4, 2, 0, 1, 1),
    ),
    11: (
        (W, 4, -1, 1), (W, 4, 0, 2), (W, 5, 0, 1), (S, 5, 0, 1, 0, -1), (S, 5, 0, 1, 0, 1),
    ),
    12: (
        (W, 5, 0, -1), (S, 5, 0, -1, 1, 1), (S, 5, 0, -1, 0, -1), (S, 5, 0, -1, 0, 1), (C, "from_sibling", 1),
    ),
    14: (
        (W, 5, 1, 0), (W, 4, -1, -1), (S, 4, -1, -1, 1, 1), (W, 4, 2, 1),
    ),
    15: (
        (W, 5, -1, 0), (S, 5, -1, 0, 0, 1),
    ),
}
DOWN_EVENTS = {
    0: (
        (W, 4, 1, 2),
    ),
    1: (
        (W, 5, 2, 0), (S, 5, 2, 0, 1, 1), (S, 5, 2, 0, 1, -1), (W, 4, -1, 2), (S, 4, -1, 2, 0, 1), (W, 5, 1, 1),
    ),
    2: (
        (W, 5, 1, -1), (S, 5, 1, -1, 1, 1), (W, 5, -1, 1), (W, 5, -1, -1), (W, 5, -1, 2), (W, 5, 1, 2),
        (S, 5, -1, 2, 0, 1), (S, 5, -1, -1, 1, 1),
    ),
    3: (
        (W, 4, 2, -1), (W, 4, 2, 2), (W, 5, 0, 2), (W, 5, 2, 1),
    ),
    4: (
        (W, 5, 2, 2), (W, 5, 2, -1),
    ),
    9: (
        (C, "drain", 0), (C, "drain", 1), (C, "drain", 2), (C, "drain", 3), (C, "drain", 6),
    ),
    10: (
        (C, "drain", 4), (C, "drain", 5),
    ),
}
LAG = 3


def kernel(tok, gain_in, gate, up, down, out, gain, wg, wd, x4, nrm, acc, hid, pb, rb, qb, mid, own, ob,
           in_sem, ssem, rsem, dsend, drecv_g, drecv_d, zsend, zrecv, tsend, trecv, psend, precv, osem):
    fs, tp = lax.axis_index("fs"), lax.axis_index("tp")
    y, x, z, c = fs // 4, fs % 4, tp // 2, tp % 2
    d = 1 - 2 * c
    par = (x + y) % 2
    pars = (par, 1 - par, par, 1 - par, 1 - par, par)
    sibling = (fs, z * 2 + 1 - c)

    def zdev(k):
        return (fs, ((z + k * d + 8) % 8) * 2 + c)

    def fpos(t, i, j):
        p = pars[t]
        yy = (y + d * (i * p + j * (1 - p)) + 8) % 4
        xx = (x + d * (i * (1 - p) + j * p) + 8) % 4
        return yy * 4 + xx

    def piece(t, core, f):
        if t < 4:
            return wg.at[core, t // 2, f, t % 2, pl.ds(0, HU), :]
        return wd.at[f, core * 2 + (t - 4), pl.ds(0, HU), :]

    def rcopy(src, dst, s, r, dev):
        return pltpu.make_async_remote_copy(
            src_ref=src, dst_ref=dst, send_sem=s, recv_sem=r, device_id=dev, device_id_type=MESH
        )

    def send(t, i, j, axis, step):
        f = fpos(t, i, j)
        ref = piece(t, c, f)
        to = fpos(t, step, 0) if axis == 0 else fpos(t, 0, step)
        rcopy(ref, ref, ssem.at[t], rsem.at[t, f], (to, tp)).start()

    def across(t, i, j):
        f = fpos(t, i, j)
        ref = piece(t, c, f)
        r = drecv_g.at[t // 2] if t < 4 else drecv_d.at[t - 4, f]
        rcopy(ref, ref, dsend.at[t], r, sibling).start()

    def got(t, i, j):
        f = fpos(t, i, j)
        ref = piece(t, c, f)
        rcopy(ref, ref, ssem.at[t], rsem.at[t, f], sibling).wait_recv()

    def own_ready(t):
        across(t, 0, 0)

    def normalize(slot):
        def rows(i, _):
            at = pl.multiple_of(i * 16, 16)
            v = x4[slot, pl.ds(at, 16), :].astype(F32)
            factor = lax.rsqrt(jnp.sum(v * v, axis=-1, keepdims=True) * (1.0 / D) + eps_floor)
            nrm[pl.ds(pl.multiple_of(slot * T + at, 16), 16), :] = (v * factor * gain[...]).astype(BF)
            return 0

        lax.fori_loop(0, T // 16, rows, 0)

    def block_of(b):
        return (1 - c if b % 2 else c), b // 2

    def matmul(b):
        core, ab = block_of(b)

        def columns(n, _):
            events_at({m: GATE_EVENTS[4 * b + m] for m in (1, 2) if 4 * b + m in GATE_EVENTS}, n)
            at = pl.ds(pl.multiple_of(n * 128, 128), 128)
            rows = [wg[core, ab, f, h, at, :] for h in (0, 1) for f in range(16)]
            w = jnp.concatenate([jnp.concatenate(rows[:16], axis=1), jnp.concatenate(rows[16:], axis=1)], axis=0)
            both = lax.dot_general(nrm[...], w, (((1,), (1,)), ((), ())), preferred_element_type=F32)
            acc[:, pl.ds(pl.multiple_of(n * 256, 256), 256)] = both
            return 0

        lax.fori_loop(0, 3, columns, 0)

    def gating(b):
        core, ab = block_of(b)
        lanes = pl.ds(pl.multiple_of((core * 2 + ab) * HP, 128), HP)

        def rows(i, _):
            at = pl.ds(pl.multiple_of(i * 32, 32), 32)
            v = acc[at, :]
            g = jnp.concatenate([v[:, n * 256 : n * 256 + 128] for n in range(3)], axis=1)
            u = jnp.concatenate([v[:, n * 256 + 128 : n * 256 + 256] for n in range(3)], axis=1)
            hid[at, lanes] = (g / (1.0 + jnp.exp(-g)) * u).astype(BF)
            return 0

        lax.fori_loop(0, 16, rows, 0)

    def from_sibling(ab):
        every = wg.at[1 - c, ab, :, :, pl.ds(0, HU), :]
        rcopy(every, every, dsend.at[ab], drecv_g.at[ab], sibling).wait_recv()

    def pair_fs(p):
        picked = []
        for h in (0, 1):
            i, j = PAIRS[0][h]
            for k in range(1, 8):
                i = jnp.where(p == k, PAIRS[k][h][0], i)
                j = jnp.where(p == k, PAIRS[k][h][1], j)
            picked.append(fpos(DOWN_A, i, j))
        return picked

    def down_pair(p):
        fa, fb = pair_fs(p)
        for t in (DOWN_A, DOWN_B):
            for f in (fa, fb):
                ref = piece(t, 1 - c, f)
                rcopy(ref, ref, dsend.at[t], drecv_d.at[t - 4, f], sibling).wait_recv()
        w = jnp.concatenate([wd[fa].reshape(4 * HP, 128), wd[fb].reshape(4 * HP, 128)], axis=1)
        part = jnp.dot(hid[...], w, preferred_element_type=F32)
        for s in (3, 2):
            for h in (0, 1):
                pb[s - 1, p, h] = part[s * T : (s + 1) * T, h * 128 : (h + 1) * 128].astype(BF)
        own[p] = part[0:T]
        mid[p] = part[T : 2 * T]
        rcopy(pb.at[2, p], qb.at[p], psend.at[2], precv.at[2, p], zdev(-1)).start()
        rcopy(pb.at[1, p], rb.at[1, p], psend.at[1], precv.at[1, p], zdev(1)).start()

    def relay(p):
        rcopy(qb.at[p], qb.at[p], psend.at[2], precv.at[2, p], sibling).wait_recv()
        for h in (0, 1):
            pb[0, p, h] = (mid[p, :, h * 128 : (h + 1) * 128] + qb[p, h].astype(F32)).astype(BF)
        rcopy(pb.at[0, p], rb.at[0, p], psend.at[0], precv.at[0, p], zdev(-1)).start()

    def finish(p):
        for s in (0, 1):
            rcopy(rb.at[s, p], rb.at[s, p], psend.at[s], precv.at[s, p], sibling).wait_recv()
        for h, f in enumerate(pair_fs(p)):
            v = own[p, :, h * 128 : (h + 1) * 128]
            for s in (0, 1):
                v = v + rb[s, p, h].astype(F32)
            ob[p, h] = v.astype(BF)
            pltpu.make_async_copy(ob.at[p, h], out.at[:, pl.ds(pl.multiple_of(f * 128, 128), 128)], osem).start()

    inputs = [
        pltpu.make_async_copy(gate, piece(GATE_A, c, fs), in_sem.at[0]),
        pltpu.make_async_copy(up, piece(UP_A, c, fs), in_sem.at[1]),
        pltpu.make_async_copy(down, piece(DOWN_A, c, fs), in_sem.at[2]),
        pltpu.make_async_copy(tok, x4.at[0], in_sem.at[3]),
        pltpu.make_async_copy(gain_in, gain, in_sem.at[4]),
    ]
    barrier = pltpu.get_barrier_semaphore()
    partners = [zdev(k) for k in (4, 1, -1)]
    partners += [(fpos(0, *o), tp) for o in ((1, 0), (-1, 0), (0, 1), (0, -1))] + [sibling]
    for dev in partners:
        pl.semaphore_signal(barrier, inc=1, device_id=dev, device_id_type=MESH)
    for cp in inputs:
        cp.start()
    for f in range(16):
        for b in range(4):
            wd[f, b, HU:HP, :] = jnp.zeros((HP - HU, 128), BF)
            for h in (0, 1):
                wg[b // 2, b % 2, f, h, HU:HP, :] = jnp.zeros((HP - HU, 128), BF)
    for cp in inputs:
        cp.wait()
    pl.semaphore_wait(barrier, len(partners))

    gz = [rcopy(piece(t, c, fs), piece(t + 2, c, fs), zsend.at[t], zrecv.at[t], zdev(4)) for t in (GATE_A, UP_A)]
    dz = rcopy(piece(DOWN_A, c, fs), piece(DOWN_B, c, fs), zsend.at[2], zrecv.at[2], zdev(4))
    t2 = rcopy(x4.at[0], x4.at[2], tsend, trecv.at[2], zdev(-1))
    t1 = rcopy(x4.at[0], x4.at[1], tsend, trecv.at[1], zdev(1))
    t3 = rcopy(x4.at[1], x4.at[3], tsend, trecv.at[3], zdev(1))

    def plane_b(k):
        (gz[0], gz[1], dz)[k].wait_recv()

    def tokens_out(k):
        for cp in ((gz[0], gz[1], t1), (t2,))[k]:
            cp.start()

    def tokens_on():
        t1.wait_recv()
        t3.start()

    def down_out():
        dz.start()

    def tokens_in(k):
        (None, None, t2, t3)[k].wait_recv()

    def drain(t):
        if t < 4:
            few = wg.at[c, t // 2, pl.ds(0, 15), t % 2, pl.ds(0, HU), :]
            all16 = wg.at[c, t // 2, :, t % 2, pl.ds(0, HU), :]
        elif t < 6:
            few = wd.at[pl.ds(0, 15), 0, pl.ds(0, HU), :]
            all16 = wd.at[:, 0, pl.ds(0, HU), :]
        else:
            for cp in (*gz, dz):
                cp.wait_send()
            three = x4.at[pl.ds(0, 3)]
            rcopy(three, three, tsend, trecv.at[1], sibling).wait_send()
            return
        rcopy(few, few, ssem.at[t], rsem.at[t, 0], sibling).wait_send()
        rcopy(all16, all16, dsend.at[t], rsem.at[t, 0], sibling).wait_send()

    tasks = {
        "own": own_ready, "plane_b": plane_b, "tokens_out": tokens_out, "tokens_on": tokens_on,
        "down_out": down_out, "tokens_in": tokens_in, "normalize": normalize, "from_sibling": from_sibling, "drain": drain,
    }

    def event(kind, *rest):
        if kind == W:
            got(*rest)
            across(*rest)
        elif kind == S:
            send(*rest)
        else:
            tasks[rest[0]](*rest[1:])

    def events_at(table, k):
        for at, some in table.items():

            @pl.when(k == at)
            def _():
                for e in some:
                    event(*e)

    for e in EVENTS:
        event(*e)

    for b in range(4):
        for e in GATE_EVENTS.get(4 * b, ()):
            event(*e)
        matmul(b)
        for e in GATE_EVENTS.get(4 * b + 3, ()):
            event(*e)
        gating(b)

    def down_step(k, _):
        events_at(DOWN_EVENTS, k)

        @pl.when(k < 8)
        def _():
            down_pair(k)

        @pl.when((k >= LAG) & (k < 8 + LAG))
        def _():
            relay(k - LAG)

        @pl.when(k >= 2 * LAG)
        def _():
            finish(k - 2 * LAG)

        return 0

    lax.fori_loop(0, 8 + 2 * LAG, down_step, 0)

    for s in range(3):
        rcopy(pb.at[s], pb.at[s], psend.at[s], precv.at[s, 0], sibling).wait_send()
    pltpu.make_async_copy(x4.at[0], out, osem).wait()


def local(tokens, norm_gain, gate_weight, up_weight, down_weight):
    hbm = pl.BlockSpec(memory_space=pl.ANY)
    dma = pltpu.SemaphoreType.DMA
    return pl.pallas_call(
        kernel,
        out_shape=jax.ShapeDtypeStruct((T, D), BF),
        in_specs=[hbm] * 5,
        out_specs=hbm,
        scratch_shapes=[
            pltpu.VMEM((1, D), F32),
            pltpu.VMEM((2, 2, 16, 2, HP, 128), BF),
            pltpu.VMEM((16, 4, HP, 128), BF),
            pltpu.VMEM((4, T, D), BF),
            pltpu.VMEM((4 * T, D), BF),
            pltpu.VMEM((4 * T, 2 * HP), F32),
            pltpu.VMEM((4 * T, 4 * HP), BF),
            pltpu.VMEM((3, 8, 2, T, 128), BF),
            pltpu.VMEM((2, 8, 2, T, 128), BF),
            pltpu.VMEM((8, 2, T, 128), BF),
            pltpu.VMEM((8, T, 256), F32),
            pltpu.VMEM((8, T, 256), F32),
            pltpu.VMEM((8, 2, T, 128), BF),
            dma((5,)),
            dma((6,)),
            dma((6, 16)),
            dma((6,)),
            dma((2,)),
            dma((2, 16)),
            dma((3,)),
            dma((3,)),
            dma(()),
            dma((4,)),
            dma((3,)),
            dma((3, 8)),
            dma(()),
        ],
        compiler_params=pltpu.CompilerParams(
            collective_id=0, has_side_effects=True, vmem_limit_bytes=58 * 2**20
        ),
    )(tokens, norm_gain.reshape(1, D), gate_weight.T, up_weight.T, down_weight)


def solution(mesh):
    return jax.shard_map(
        local,
        mesh=mesh,
        in_specs=(P(("fs", "tp"), None), P(), P("fs", "tp"), P("fs", "tp"), P("tp", "fs")),
        out_specs=P(("fs", "tp"), None),
        check_vma=False,
    )
```

```python
import jax
import jax.numpy as jnp
from jax import lax
from jax.experimental import pallas as pl
from jax.experimental.pallas import tpu as pltpu
from jax.sharding import PartitionSpec as P

MESH = pl.DeviceIdType.MESH
BF, F32 = jnp.bfloat16, jnp.float32
eps_floor = 0.05

D, T, HU, HP = 2048, 128, 352, 384
GATE_A, UP_A, GATE_B, UP_B, DOWN_A, DOWN_B = range(6)
PAIRS = (((0, 0), (-1, 0)), ((1, 0), (0, -1)), ((0, 1), (0, 2)), ((-1, 1), (1, -1)), ((-1, -1), (1, 1)), ((2, -1), (2, 1)), ((2, 0), (-1, 2)), ((1, 2), (2, 2)))
W, S, C = 0, 1, 2
EVENTS = (
    (C, "own", 0), (C, "own", 1), (C, "own", 4), (S, 0, 0, 0, 0, 1), (S, 0, 0, 0, 0, -1), (S, 0, 0, 0, 1, 1),
    (S, 0, 0, 0, 1, -1), (S, 1, 0, 0, 1, 1), (S, 1, 0, 0, 1, -1), (S, 1, 0, 0, 0, 1), (S, 1, 0, 0, 0, -1),
    (S, 4, 0, 0, 0, -1), (C, "tokens_out", 0), (S, 4, 0, 0, 1, -1), (W, 0, 0, -1), (W, 0, 0, 1), (W, 0, -1, 0),
    (W, 0, 1, 0), (S, 0, 0, -1, 0, 1), (S, 0, 0, -1, 0, -1), (S, 0, 0, -1, 1, 1), (S, 0, 0, 1, 0, 1),
    (S, 0, 0, 1, 0, -1), (S, 0, -1, 0, 0, 1), (C, "normalize", 0), (W, 1, -1, 0), (W, 1, 1, 0), (W, 1, 0, -1),
    (W, 1, 0, 1), (S, 1, -1, 0, 0, 1), (S, 1, 0, -1, 0, -1), (S, 1, 0, -1, 0, 1), (S, 1, 0, 1, 0, -1),
    (S, 1, 0, -1, 1, 1), (S, 1, 0, 1, 0, 1), (W, 0, -1, -1), (W, 0, -1, 1), (W, 0, 2, 0), (W, 4, 0, 1),
    (S, 0, 2, 0, 1, -1), (S, 0, -1, -1, 1, 1), (S, 0, 2, 0, 1, 1), (W, 0, 1, -1), (W, 0, 1, 1), (W, 1, 0, 2),
    (W, 1, -1, 1), (S, 0, 1, -1, 1, 1), (S, 4, 0, 1, 0, -1), (C, "plane_b", 0), (C, "own", 2), (C, "plane_b", 1),
    (C, "own", 3), (S, 2, 0, 0, 0, -1), (S, 2, 0, 0, 0, 1), (S, 2, 0, 0, 1, -1), (S, 3, 0, 0, 1, -1),
    (S, 3, 0, 0, 0, -1), (S, 2, 0, 0, 1, 1), (S, 3, 0, 0, 1, 1), (S, 3, 0, 0, 0, 1), (C, "tokens_out", 1),
    (W, 0, 0, 2), (W, 4, 1, 0), (W, 1, -1, -1), (W, 1, 1, 1), (S, 1, -1, -1, 1, 1), (W, 1, 2, 0),
    (S, 1, 2, 0, 1, -1), (S, 1, 2, 0, 1, 1), (W, 1, 1, -1), (W, 0, 1, 2), (S, 1, 1, -1, 1, 1), (W, 2, 0, 1),
    (S, 2, 0, 1, 0, -1), (S, 2, 0, 1, 0, 1), (W, 2, 0, -1), (S, 2, 0, -1, 0, -1), (S, 2, 0, -1, 1, 1),
    (S, 2, 0, -1, 0, 1), (W, 0, 2, -1), (W, 2, 1, 0), (C, "tokens_on"), (W, 3, 1, 0), (W, 1, 2, -1),
    (C, "normalize", 1), (W, 0, -1, 2), (W, 3, 0, 1), (S, 3, 0, 1, 0, -1), (S, 0, -1, 2, 0, 1), (S, 3, 0, 1, 0, 1),
    (W, 1, 1, 2), (W, 1, -1, 2), (S, 1, -1, 2, 0, 1), (W, 0, 2, 1), (W, 4, 1, 1), (W, 2, 1, 1), (W, 1, 2, 1),
    (S, 4, 0, 0, 1, 1), (W, 2, -1, 0), (W, 3, 1, 1), (S, 2, -1, 0, 0, 1), (W, 2, -1, 1), (W, 0, 2, 2), (W, 1, 2, 2),
    (C, "down_out"), (W, 3, -1, 0), (W, 3, 0, -1), (S, 3, 0, -1, 0, -1), (S, 3, -1, 0, 0, 1), (S, 3, 0, -1, 1, 1),
    (S, 3, 0, -1, 0, 1), (W, 2, 1, -1), (W, 2, 2, 0), (S, 2, 2, 0, 1, -1), (S, 2, 1, -1, 1, 1), (S, 2, 2, 0, 1, 1),
    (S, 4, 0, 0, 0, 1), (W, 2, -1, -1), (S, 2, -1, -1, 1, 1), (W, 3, 1, -1), (S, 3, 1, -1, 1, 1), (W, 2, 0, 2),
    (S, 4, 0, 1, 0, 1), (W, 3, -1, 1), (W, 3, 2, 0), (S, 3, 2, 0, 1, -1), (S, 3, 2, 0, 1, 1), (W, 3, 0, 2),
    (C, "tokens_in", 2), (C, "normalize", 2), (W, 3, 2, 1), (C, "tokens_in", 3), (C, "normalize", 3), (W, 2, 1, 2),
    (W, 3, -1, -1), (S, 3, -1, -1, 1, 1), (W, 4, -1, 0), (S, 4, -1, 0, 0, 1),
)
GATE_EVENTS = {
    1: (
        (W, 2, 2, 1),
    ),
    2: (
        (W, 3, 1, 2), (W, 3, -1, 2), (W, 2, -1, 2), (S, 2, -1, 2, 0, 1), (S, 3, -1, 2, 0, 1),
    ),
    4: (
        (W, 3, 2, -1), (W, 2, 2, -1), (C, "from_sibling", 0),
    ),
    5: (
        (W, 4, 0, -1), (S, 4, 0, -1, 1, 1), (S, 4, 0, -1, 0, -1), (S, 4, 0, -1, 0, 1),
    ),
    6: (
        (C, "plane_b", 2), (C, "own", 5), (S, 5, 0, 0, 0, -1), (S, 5, 0, 0, 0, 1), (S, 5, 0, 0, 1, -1),
        (S, 5, 0, 0, 1, 1),
    ),
    7: (
        (W, 2, 2, 2), (W, 3, 2, 2),
    ),
    8: (
        (W, 4, 1, -1), (S, 4, 1, -1, 1, 1),
    ),
    10: (
        (W, 4, 2, 0), (S, 4, 2, 0, 1, -1), (S, 4, 2, 0, 1, 1),
    ),
    11: (
        (W, 4, -1, 1), (W, 4, 0, 2), (W, 5, 0, 1), (S, 5, 0, 1, 0, -1), (S, 5, 0, 1, 0, 1),
    ),
    12: (
        (W, 5, 0, -1), (S, 5, 0, -1, 1, 1), (S, 5, 0, -1, 0, -1), (S, 5, 0, -1, 0, 1), (C, "from_sibling", 1),
    ),
    14: (
        (W, 5, 1, 0), (W, 4, -1, -1), (S, 4, -1, -1, 1, 1), (W, 4, 2, 1),
    ),
    15: (
        (W, 5, -1, 0), (S, 5, -1, 0, 0, 1),
    ),
}
DOWN_EVENTS = {
    0: (
        (W, 4, 1, 2),
    ),
    1: (
        (W, 5, 2, 0), (S, 5, 2, 0, 1, 1), (S, 5, 2, 0, 1, -1), (W, 4, -1, 2), (S, 4, -1, 2, 0, 1), (W, 5, 1, 1),
    ),
    2: (
        (W, 5, 1, -1), (S, 5, 1, -1, 1, 1), (W, 5, -1, 1), (W, 5, -1, -1), (W, 5, -1, 2), (W, 5, 1, 2),
        (S, 5, -1, 2, 0, 1), (S, 5, -1, -1, 1, 1),
    ),
    3: (
        (W, 4, 2, -1), (W, 4, 2, 2), (W, 5, 0, 2), (W, 5, 2, 1),
    ),
    4: (
        (W, 5, 2, 2), (W, 5, 2, -1),
    ),
    9: (
        (C, "drain", 0), (C, "drain", 1), (C, "drain", 2), (C, "drain", 3), (C, "drain", 6),
    ),
    10: (
        (C, "drain", 4), (C, "drain", 5),
    ),
}
LAG = 4


def kernel(tok, gain_in, gate, up, down, out, gain, wg, wd, x4, nrm, acc, hid, pb, rb, qb, mid, own, ob,
           in_sem, ssem, rsem, dsend, drecv_g, drecv_d, zsend, zrecv, tsend, trecv, psend, precv, osem):
    fs, tp = lax.axis_index("fs"), lax.axis_index("tp")
    y, x, z, c = fs // 4, fs % 4, tp // 2, tp % 2
    d = 1 - 2 * c
    par = (x + y) % 2
    pars = (par, 1 - par, par, 1 - par, 1 - par, par)
    sibling = (fs, z * 2 + 1 - c)

    def zdev(k):
        return (fs, ((z + k * d + 8) % 8) * 2 + c)

    def fpos(t, i, j):
        p = pars[t]
        yy = (y + d * (i * p + j * (1 - p)) + 8) % 4
        xx = (x + d * (i * (1 - p) + j * p) + 8) % 4
        return yy * 4 + xx

    def piece(t, core, f):
        if t < 4:
            return wg.at[core, t // 2, f, t % 2, pl.ds(0, HU), :]
        return wd.at[f, core * 2 + (t - 4), pl.ds(0, HU), :]

    def rcopy(src, dst, s, r, dev):
        return pltpu.make_async_remote_copy(
            src_ref=src, dst_ref=dst, send_sem=s, recv_sem=r, device_id=dev, device_id_type=MESH
        )

    def send(t, i, j, axis, step):
        f = fpos(t, i, j)
        ref = piece(t, c, f)
        to = fpos(t, step, 0) if axis == 0 else fpos(t, 0, step)
        rcopy(ref, ref, ssem.at[t], rsem.at[t, f], (to, tp)).start()

    def across(t, i, j):
        f = fpos(t, i, j)
        ref = piece(t, c, f)
        r = drecv_g.at[t // 2] if t < 4 else drecv_d.at[t - 4, f]
        rcopy(ref, ref, dsend.at[t], r, sibling).start()

    def got(t, i, j):
        f = fpos(t, i, j)
        ref = piece(t, c, f)
        rcopy(ref, ref, ssem.at[t], rsem.at[t, f], sibling).wait_recv()

    def own_ready(t):
        across(t, 0, 0)

    def normalize(slot):
        def rows(i, _):
            at = pl.multiple_of(i * 16, 16)
            v = x4[slot, pl.ds(at, 16), :].astype(F32)
            factor = lax.rsqrt(jnp.sum(v * v, axis=-1, keepdims=True) * (1.0 / D) + eps_floor)
            nrm[pl.ds(pl.multiple_of(slot * T + at, 16), 16), :] = (v * factor * gain[...]).astype(BF)
            return 0

        lax.fori_loop(0, T // 16, rows, 0)

    def block_of(b):
        return (1 - c if b % 2 else c), b // 2

    def matmul(b):
        core, ab = block_of(b)

        def columns(n, _):
            events_at({m: GATE_EVENTS[4 * b + m] for m in (1, 2) if 4 * b + m in GATE_EVENTS}, n)
            at = pl.ds(pl.multiple_of(n * 128, 128), 128)
            rows = [wg[core, ab, f, h, at, :] for h in (0, 1) for f in range(16)]
            w = jnp.concatenate([jnp.concatenate(rows[:16], axis=1), jnp.concatenate(rows[16:], axis=1)], axis=0)
            both = lax.dot_general(nrm[...], w, (((1,), (1,)), ((), ())), preferred_element_type=F32)
            acc[:, pl.ds(pl.multiple_of(n * 256, 256), 256)] = both
            return 0

        lax.fori_loop(0, 3, columns, 0)

    def gating(b):
        core, ab = block_of(b)
        lanes = pl.ds(pl.multiple_of((core * 2 + ab) * HP, 128), HP)

        def rows(i, _):
            at = pl.ds(pl.multiple_of(i * 32, 32), 32)
            v = acc[at, :]
            g = jnp.concatenate([v[:, n * 256 : n * 256 + 128] for n in range(3)], axis=1)
            u = jnp.concatenate([v[:, n * 256 + 128 : n * 256 + 256] for n in range(3)], axis=1)
            hid[at, lanes] = (g / (1.0 + jnp.exp(-g)) * u).astype(BF)
            return 0

        lax.fori_loop(0, 16, rows, 0)

    def from_sibling(ab):
        every = wg.at[1 - c, ab, :, :, pl.ds(0, HU), :]
        rcopy(every, every, dsend.at[ab], drecv_g.at[ab], sibling).wait_recv()

    def pair_fs(p):
        picked = []
        for h in (0, 1):
            i, j = PAIRS[0][h]
            for k in range(1, 8):
                i = jnp.where(p == k, PAIRS[k][h][0], i)
                j = jnp.where(p == k, PAIRS[k][h][1], j)
            picked.append(fpos(DOWN_A, i, j))
        return picked

    def down_pair(p):
        fa, fb = pair_fs(p)
        for t in (DOWN_A, DOWN_B):
            for f in (fa, fb):
                ref = piece(t, 1 - c, f)
                rcopy(ref, ref, dsend.at[t], drecv_d.at[t - 4, f], sibling).wait_recv()
        w = jnp.concatenate([wd[fa].reshape(4 * HP, 128), wd[fb].reshape(4 * HP, 128)], axis=1)
        part = jnp.dot(hid[...], w, preferred_element_type=F32)
        for s in (3, 2):
            for h in (0, 1):
                pb[s - 1, p, h] = part[s * T : (s + 1) * T, h * 128 : (h + 1) * 128].astype(BF)
        own[p] = part[0:T]
        mid[p] = part[T : 2 * T]
        rcopy(pb.at[2, p], qb.at[p], psend.at[2], precv.at[2, p], zdev(-1)).start()
        rcopy(pb.at[1, p], rb.at[1, p], psend.at[1], precv.at[1, p], zdev(1)).start()

    def relay(p):
        rcopy(qb.at[p], qb.at[p], psend.at[2], precv.at[2, p], sibling).wait_recv()
        for h in (0, 1):
            pb[0, p, h] = (mid[p, :, h * 128 : (h + 1) * 128] + qb[p, h].astype(F32)).astype(BF)
        rcopy(pb.at[0, p], rb.at[0, p], psend.at[0], precv.at[0, p], zdev(-1)).start()

    def finish(p):
        for s in (0, 1):
            rcopy(rb.at[s, p], rb.at[s, p], psend.at[s], precv.at[s, p], sibling).wait_recv()
        for h, f in enumerate(pair_fs(p)):
            v = own[p, :, h * 128 : (h + 1) * 128]
            for s in (0, 1):
                v = v + rb[s, p, h].astype(F32)
            ob[p, h] = v.astype(BF)
            pltpu.make_async_copy(ob.at[p, h], out.at[:, pl.ds(pl.multiple_of(f * 128, 128), 128)], osem).start()

    inputs = [
        pltpu.make_async_copy(gate, piece(GATE_A, c, fs), in_sem.at[0]),
        pltpu.make_async_copy(up, piece(UP_A, c, fs), in_sem.at[1]),
        pltpu.make_async_copy(down, piece(DOWN_A, c, fs), in_sem.at[2]),
        pltpu.make_async_copy(tok, x4.at[0], in_sem.at[3]),
        pltpu.make_async_copy(gain_in, gain, in_sem.at[4]),
    ]
    barrier = pltpu.get_barrier_semaphore()
    partners = [zdev(k) for k in (4, 1, -1)]
    partners += [(fpos(0, *o), tp) for o in ((1, 0), (-1, 0), (0, 1), (0, -1))] + [sibling]
    for dev in partners:
        pl.semaphore_signal(barrier, inc=1, device_id=dev, device_id_type=MESH)
    for cp in inputs:
        cp.start()
    for f in range(16):
        for b in range(4):
            wd[f, b, HU:HP, :] = jnp.zeros((HP - HU, 128), BF)
            for h in (0, 1):
                wg[b // 2, b % 2, f, h, HU:HP, :] = jnp.zeros((HP - HU, 128), BF)
    for cp in inputs:
        cp.wait()
    pl.semaphore_wait(barrier, len(partners))

    gz = [rcopy(piece(t, c, fs), piece(t + 2, c, fs), zsend.at[t], zrecv.at[t], zdev(4)) for t in (GATE_A, UP_A)]
    dz = rcopy(piece(DOWN_A, c, fs), piece(DOWN_B, c, fs), zsend.at[2], zrecv.at[2], zdev(4))
    t2 = rcopy(x4.at[0], x4.at[2], tsend, trecv.at[2], zdev(-1))
    t1 = rcopy(x4.at[0], x4.at[1], tsend, trecv.at[1], zdev(1))
    t3 = rcopy(x4.at[1], x4.at[3], tsend, trecv.at[3], zdev(1))

    def plane_b(k):
        (gz[0], gz[1], dz)[k].wait_recv()

    def tokens_out(k):
        for cp in ((gz[0], gz[1], t1), (t2,))[k]:
            cp.start()

    def tokens_on():
        t1.wait_recv()
        t3.start()

    def down_out():
        dz.start()

    def tokens_in(k):
        (None, None, t2, t3)[k].wait_recv()

    def drain(t):
        if t < 4:
            few = wg.at[c, t // 2, pl.ds(0, 15), t % 2, pl.ds(0, HU), :]
            all16 = wg.at[c, t // 2, :, t % 2, pl.ds(0, HU), :]
        elif t < 6:
            few = wd.at[pl.ds(0, 15), 0, pl.ds(0, HU), :]
            all16 = wd.at[:, 0, pl.ds(0, HU), :]
        else:
            for cp in (*gz, dz):
                cp.wait_send()
            three = x4.at[pl.ds(0, 3)]
            rcopy(three, three, tsend, trecv.at[1], sibling).wait_send()
            return
        rcopy(few, few, ssem.at[t], rsem.at[t, 0], sibling).wait_send()
        rcopy(all16, all16, dsend.at[t], rsem.at[t, 0], sibling).wait_send()

    tasks = {
        "own": own_ready, "plane_b": plane_b, "tokens_out": tokens_out, "tokens_on": tokens_on,
        "down_out": down_out, "tokens_in": tokens_in, "normalize": normalize, "from_sibling": from_sibling, "drain": drain,
    }

    def event(kind, *rest):
        if kind == W:
            got(*rest)
            across(*rest)
        elif kind == S:
            send(*rest)
        else:
            tasks[rest[0]](*rest[1:])

    def events_at(table, k):
        for at, some in table.items():

            @pl.when(k == at)
            def _():
                for e in some:
                    event(*e)

    for e in EVENTS:
        event(*e)

    for b in range(4):
        for e in GATE_EVENTS.get(4 * b, ()):
            event(*e)
        matmul(b)
        for e in GATE_EVENTS.get(4 * b + 3, ()):
            event(*e)
        gating(b)

    def down_step(k, _):
        events_at(DOWN_EVENTS, k)

        @pl.when(k < 8)
        def _():
            down_pair(k)

        @pl.when((k >= LAG) & (k < 8 + LAG))
        def _():
            relay(k - LAG)

        @pl.when(k >= 2 * LAG)
        def _():
            finish(k - 2 * LAG)

        return 0

    lax.fori_loop(0, 8 + 2 * LAG, down_step, 0)

    for s in range(3):
        rcopy(pb.at[s], pb.at[s], psend.at[s], precv.at[s, 0], sibling).wait_send()
    pltpu.make_async_copy(x4.at[0], out, osem).wait()


def local(tokens, norm_gain, gate_weight, up_weight, down_weight):
    hbm = pl.BlockSpec(memory_space=pl.ANY)
    dma = pltpu.SemaphoreType.DMA
    return pl.pallas_call(
        kernel,
        out_shape=jax.ShapeDtypeStruct((T, D), BF),
        in_specs=[hbm] * 5,
        out_specs=hbm,
        scratch_shapes=[
            pltpu.VMEM((1, D), F32),
            pltpu.VMEM((2, 2, 16, 2, HP, 128), BF),
            pltpu.VMEM((16, 4, HP, 128), BF),
            pltpu.VMEM((4, T, D), BF),
            pltpu.VMEM((4 * T, D), BF),
            pltpu.VMEM((4 * T, 2 * HP), F32),
            pltpu.VMEM((4 * T, 4 * HP), BF),
            pltpu.VMEM((3, 8, 2, T, 128), BF),
            pltpu.VMEM((2, 8, 2, T, 128), BF),
            pltpu.VMEM((8, 2, T, 128), BF),
            pltpu.VMEM((8, T, 256), F32),
            pltpu.VMEM((8, T, 256), F32),
            pltpu.VMEM((8, 2, T, 128), BF),
            dma((5,)),
            dma((6,)),
            dma((6, 16)),
            dma((6,)),
            dma((2,)),
            dma((2, 16)),
            dma((3,)),
            dma((3,)),
            dma(()),
            dma((4,)),
            dma((3,)),
            dma((3, 8)),
            dma(()),
        ],
        compiler_params=pltpu.CompilerParams(
            collective_id=0, has_side_effects=True, vmem_limit_bytes=58 * 2**20
        ),
    )(tokens, norm_gain.reshape(1, D), gate_weight.T, up_weight.T, down_weight)


def solution(mesh):
    return jax.shard_map(
        local,
        mesh=mesh,
        in_specs=(P(("fs", "tp"), None), P(), P("fs", "tp"), P("fs", "tp"), P("tp", "fs")),
        out_specs=P(("fs", "tp"), None),
        check_vma=False,
    )
```
